32 devices in a mesh: grp: 2 (over y), kv: 4 (over z), tp: 4 (over x, core).
Axes of the slice: x: 2, y: 2, z: 4, core: 2. Of those that a mesh axis runs over, the one named last changes fastest.
Arguments:
- tokens: bfloat16 [48, 4096], P('grp', ('kv', 'tp')), parts along dimension 0, may hold values from -30 to 30
- norm_gain: bfloat16 [4096], P(('kv', 'tp')), may hold values from 0.099609375 to 1.8984375
- query_weight: bfloat16 [4096, 4096], P('kv', 'tp'), may hold values from -0.09375 to 0.09375
- key_weight: bfloat16 [4096, 4096], P('kv', 'tp'), may hold values from -0.5 to 0.5
- value_weight: bfloat16 [4096, 4096], P('kv', 'tp'), may hold values from -0.09375 to 0.09375
- lambda_head: float32 [16], P('tp'), may hold values from 0.3 to 0.8
- head_gain: float32 [256], replicated, may hold values from 0.1 to 1.9
- out_weight: bfloat16 [4096, 4096], P('tp', 'kv'), may hold values from -0.09375 to 0.09375
- cache_keys: bfloat16 [48, 256, 4096], P('grp', 'kv', 'tp'), parts along dimension 0, may hold values from -300 to 300
- cache_values: bfloat16 [48, 256, 4096], P('grp', 'kv', 'tp'), parts along dimension 0, may hold values from -6 to 6
- lengths: int32 [48], P('grp'), parts along dimension 0, may hold values from 64 to 255, as said below
Outputs:
- layer_out: bfloat16 [48, 4096], P('grp', ('kv', 'tp')), parts along dimension 0
- log_sums: float32 [48, 16, 2], P('grp', 'tp'), parts along dimension 0
The draws below stay inside these ranges and needn't reach their ends.
There are 2 independent parts, one for each index of `grp`. The reference program is written for one: setup_inputs(seed, part) draws one part's arguments, and reference() takes and returns one part's arrays. A program takes and returns all parts, laid end to end along the dimension named above; an argument that names none is the same for every part. Nothing has to cross between parts.
Inputs may be any that keep to these rules, and one draw needn't show every extreme that they name: The new token of sequence b goes to cache position lengths[b]; in every draw some sequence has the largest length allowed.
All inputs are finite; a program needn't handle non-finite values.
Results may differ from the reference program's by a relative error of at most 0.017.
The reference program's roundings to bfloat16 on the way (of `scaled`, `queries`, `key_new`, `value_new`, `keys_all`, `values_all`, `weights_low` and `attended`) count: a program that leaves them out, or rounds other values in their place, can miss the bound.
Values may be sent and summed in bfloat16 or wider, within the bound.
A program may use at most 64 MiB of HBM per device.

```python
import math
import jax
import jax.numpy as jnp
from jax import lax

D = 4096
HEADS = 16
HEAD_DIM = 128
VALUE_DIM = 256
BATCH = 24
POS_DEV = 64
CACHE = 256
N_TP = 4


def draw_tokens(key, part):
    key_base, key_block, key_row = jax.random.split(key, 3)
    block_width = D // 128
    base = jnp.clip(jax.random.normal(key_base, (BATCH, D), jnp.float32), -5.0, 5.0)
    block_scale = jnp.exp(jax.random.uniform(key_block, (128,), jnp.float32, math.log(0.33), math.log(3.0)))
    row_scale = jnp.exp(jax.random.uniform(key_row, (BATCH, 1), jnp.float32, math.log(0.5), math.log(2.0)))
    column_scale = jnp.repeat(block_scale, block_width)
    return (base * column_scale[None, :] * row_scale).astype(jnp.bfloat16)


def draw_cache_keys(key, part):
    shape = (BATCH, CACHE, 2 * HEADS * HEAD_DIM)
    base = jnp.clip(jax.random.normal(key, shape, jnp.float32) * 1.75, -10.5, 10.5)
    return base.astype(jnp.bfloat16)


def draw_lengths(key, part):
    key_base, key_pick = jax.random.split(key, 2)
    base = jax.random.randint(key_base, (BATCH,), CACHE // 4, CACHE)
    chosen = jax.random.randint(key_pick, (), 0, BATCH)
    return jnp.where(jnp.arange(BATCH) == chosen, CACHE - 1, base).astype(jnp.int32)


def level_of(stream_key, dims, pieces, smallest, largest):
    def one(axis_at, blocks):
        heights = jax.random.uniform(jax.random.fold_in(jax.random.fold_in(stream_key, 6), axis_at), (blocks,), jnp.float32, smallest / len(pieces), largest / len(pieces))
        return jnp.repeat(jnp.exp(heights), dims[axis_at] // blocks).reshape((-1,) + (1,) * (len(dims) - axis_at - 1))

    level = one(*pieces[0])
    for cut in pieces[1:]:
        level = level * one(*cut)
    return level


def noise(stream_key, extent, width, most, cuts=(), held_as=jnp.bfloat16):
    gain = level_of(stream_key, extent, cuts, -0.22, 0.18) if cuts else 1.0
    result = jax.random.normal(stream_key, extent, jnp.float32) * width * gain
    return jnp.minimum(jnp.maximum(result, -most), most).astype(held_as)


def setup_inputs(seed: int = 0, part: int = 0) -> dict:
    key_of = jax.random.split(jax.random.key(seed), 12)
    own_keys = jax.random.split(jax.random.fold_in(key_of[11], part), 12)
    return {
        "tokens": draw_tokens(jax.random.fold_in(jax.random.fold_in(key_of[11], part), 71), part),
        "norm_gain": jnp.clip(1.0 + 0.18 * jax.random.normal(key_of[1], (D,), jnp.float32), 0.099609375, 1.8984375).astype(jnp.bfloat16),
        "query_weight": noise(key_of[2], (D, 2 * HEADS * HEAD_DIM), D ** -0.5, 0.09375, ((0, 4), (1, 4))),
        "key_weight": noise(key_of[3], (D, 2 * HEADS * HEAD_DIM), (D // 32) ** -0.5, 0.5, ((0, 4), (1, 4))),
        "value_weight": noise(key_of[4], (D, HEADS * VALUE_DIM), D ** -0.5, 0.09375, ((0, 4), (1, 4))),
        "lambda_head": jnp.clip(0.3 + 0.5 * jax.random.uniform(key_of[5], (HEADS,), jnp.float32) ** level_of(key_of[5], (HEADS,), ((0, 4),), -0.2, 0.2), 0.3, 0.8),
        "head_gain": jnp.clip(1.0 + 0.18 * jax.random.normal(key_of[6], (VALUE_DIM,), jnp.float32), 0.1, 1.9),
        "out_weight": noise(key_of[7], (HEADS * VALUE_DIM, D), (HEADS * VALUE_DIM) ** -0.5, 0.09375, ((0, 4), (1, 4))),
        "cache_keys": draw_cache_keys(jax.random.fold_in(jax.random.fold_in(key_of[11], part), 71), part),
        "cache_values": noise(own_keys[9], (BATCH, CACHE, HEADS * VALUE_DIM), 1.0, 6.0, ((1, 4), (2, 4))),
        "lengths": draw_lengths(jax.random.fold_in(jax.random.fold_in(key_of[11], part), 71), part),
    }


def rotate(vectors, lengths):
    half_dim = vectors.shape[-1] // 2
    freqs = jnp.power(jnp.float32(500000.0), -(jnp.arange(half_dim, dtype=jnp.float32) * 2.0 / vectors.shape[-1]))
    angles = lengths.astype(jnp.float32)[:, None] * freqs[None, :]
    cosine = jnp.cos(angles)[:, None, None, :]
    sine = jnp.sin(angles)[:, None, None, :]
    lower = vectors[..., :half_dim]
    upper = vectors[..., half_dim:]
    return jnp.concatenate([lower * cosine - upper * sine, upper * cosine + lower * sine], axis=-1)

def project(scaled, weight, inv_rms):
    return jnp.dot(scaled, weight, preferred_element_type=jnp.float32) * inv_rms[:, None]

def attend_one(packed):
    query_row, key_row, value_row, keys, values, length = packed
    total_len = keys.shape[0]
    positions = jnp.arange(total_len, dtype=jnp.int32)
    new_slot = positions == length
    keys_all = jnp.where(new_slot[:, None], key_row[None, :], keys)
    values_all = jnp.where(new_slot[:, None], value_row[None, :], values)
    keys_four = keys_all.reshape(total_len, HEADS, 2, HEAD_DIM)
    query_three = query_row.reshape(HEADS, 2, HEAD_DIM)
    scores = jnp.einsum('hcd,phcd->hcp', query_three.astype(jnp.float32), keys_four.astype(jnp.float32)) * HEAD_DIM ** (-0.5)
    nblocks = total_len // POS_DEV
    scores = scores.reshape(HEADS, 2, nblocks, POS_DEV)
    visible = (positions <= length).reshape(nblocks, POS_DEV)
    block_max = lax.optimization_barrier(jnp.max(jnp.where(visible, scores, -1e+30), axis=-1))
    weights = jnp.where(visible, jnp.exp(scores - block_max[..., None]), 0.0)
    block_sum = lax.optimization_barrier(jnp.sum(weights, axis=-1))
    weights_low = lax.optimization_barrier(weights.astype(jnp.bfloat16))
    values_four = values_all.reshape(nblocks, POS_DEV, HEADS, VALUE_DIM)
    block_out = jnp.einsum('hcnp,nphe->hcne', weights_low.astype(jnp.float32), values_four.astype(jnp.float32))
    row_max = lax.optimization_barrier(jnp.max(block_max, axis=-1))
    factor = jnp.exp(block_max - row_max[..., None])
    weight_total = lax.optimization_barrier(jnp.sum(block_sum * factor, axis=-1))
    combined = lax.optimization_barrier(jnp.sum(block_out * factor[..., None], axis=2))
    return (combined, weight_total, row_max)

def reference(tokens, norm_gain, query_weight, key_weight, value_weight, lambda_head, head_gain, out_weight, cache_keys, cache_values, lengths):
    seq_count = tokens.shape[0]
    tok_float = tokens.astype(jnp.float32)
    row_squares = lax.optimization_barrier(jnp.sum(tok_float * tok_float, axis=1))
    inv_rms = lax.rsqrt(row_squares / D + 1e-06)
    scaled = (tok_float * norm_gain.astype(jnp.float32)).astype(jnp.bfloat16)
    query_sum = project(scaled, query_weight, inv_rms).reshape(seq_count, HEADS, 2, HEAD_DIM)
    key_sum = project(scaled, key_weight, inv_rms).reshape(seq_count, HEADS, 2, HEAD_DIM)
    value_sum = project(scaled, value_weight, inv_rms)
    queries = lax.optimization_barrier(rotate(query_sum, lengths).astype(jnp.bfloat16))
    key_new = rotate(key_sum, lengths).astype(jnp.bfloat16)
    value_new = value_sum.astype(jnp.bfloat16)
    combined, weight_total, row_max = lax.map(attend_one, (queries.reshape(seq_count, -1), key_new.reshape(seq_count, -1), value_new, cache_keys, cache_values, lengths))
    log_sums = row_max + jnp.log(weight_total)
    map_out = combined / weight_total[..., None]
    difference = map_out[:, :, 0] - lambda_head[None, :, None] * map_out[:, :, 1]
    inv_head = lax.rsqrt(lax.optimization_barrier(jnp.mean(difference * difference, axis=-1, keepdims=True)) + 1e-05)
    attended = (difference * inv_head * head_gain).astype(jnp.bfloat16).reshape(seq_count, HEADS * VALUE_DIM)
    attended = lax.optimization_barrier(attended)
    partial_value = jnp.einsum('bgk,gkd->gbd', attended.reshape(seq_count, N_TP, -1).astype(jnp.float32), out_weight.reshape(N_TP, -1, D).astype(jnp.float32))
    partial_value = lax.optimization_barrier(partial_value.astype(jnp.bfloat16))
    layer_out = lax.optimization_barrier(jnp.sum(partial_value.astype(jnp.float32), axis=0)).astype(jnp.bfloat16)
    return (layer_out, log_sums)
```

```python
import functools
import math

import jax
import jax.numpy as jnp
from jax import lax
from jax.experimental import pallas as pl
from jax.experimental.pallas import tpu as pltpu
from jax.sharding import PartitionSpec as P

D = 4096
HEAD_DIM = 128
VALUE_DIM = 256


def merged(part, axis, combine):
    gathered = jax.tree.map(lambda a: lax.all_gather(a, axis), part)

    def take(source):
        return jax.tree.map(lambda a: lax.dynamic_index_in_dim(a, source, 0, False), gathered)

    return lax.fori_loop(
        1, lax.axis_size(axis), lambda source, state: combine(state, take(source)), take(0)
    )


def rotate(vectors, lengths):
    half_dim = vectors.shape[-1] // 2
    freqs = jnp.power(
        jnp.float32(500000.0), -(jnp.arange(half_dim, dtype=jnp.float32) * 2.0 / vectors.shape[-1])
    )
    angles = lengths.astype(jnp.float32)[:, None] * freqs[None, :]
    cosine = jnp.cos(angles)[:, None, None, :]
    sine = jnp.sin(angles)[:, None, None, :]
    lower = vectors[..., :half_dim]
    upper = vectors[..., half_dim:]
    return jnp.concatenate([lower * cosine - upper * sine, upper * cosine + lower * sine], axis=-1)


def fold_maps(left_part, right_part):
    left_max, left_sum, left_out = left_part
    right_max, right_sum, right_out = right_part
    joint = jnp.maximum(left_max, right_max)
    left_scale = jnp.exp(left_max - joint)
    right_scale = jnp.exp(right_max - joint)
    return (
        joint,
        left_sum * left_scale + right_sum * right_scale,
        left_out * left_scale[..., None] + right_out * right_scale[..., None],
    )


def on_device(
    tokens,
    norm_gain,
    query_weight,
    key_weight,
    value_weight,
    lambda_head,
    head_gain,
    out_weight,
    cache_keys,
    cache_values,
    lengths,
):
    seq_count = tokens.shape[0]
    heads_loc = lambda_head.shape[0]
    token_block, gain_block = (
        lax.all_gather(tokens, "tp", axis=1, tiled=True),
        lax.all_gather(norm_gain, "tp", axis=0, tiled=True),
    )
    tok_float = token_block.astype(jnp.float32)
    scaled = (tok_float * gain_block.astype(jnp.float32)).astype(jnp.bfloat16)
    query_part = jnp.dot(scaled, query_weight, preferred_element_type=jnp.float32)
    key_part = jnp.dot(scaled, key_weight, preferred_element_type=jnp.float32)
    value_part = jnp.dot(scaled, value_weight, preferred_element_type=jnp.float32)
    local_squares = jnp.sum(tok_float * tok_float, axis=1)
    query_sum, key_sum, value_sum, row_squares = lax.psum(
        (query_part, key_part, value_part, local_squares), "kv"
    )
    inv_rms = lax.rsqrt(row_squares / D + 1e-06)[:, None]
    queries = rotate(
        (query_sum * inv_rms).reshape(seq_count, heads_loc, 2, HEAD_DIM), lengths
    ).astype(jnp.bfloat16)
    key_new = rotate(
        (key_sum * inv_rms).reshape(seq_count, heads_loc, 2, HEAD_DIM), lengths
    ).astype(jnp.bfloat16)
    value_new = (value_sum * inv_rms).astype(jnp.bfloat16).reshape(seq_count, heads_loc, VALUE_DIM)
    span_len = cache_keys.shape[1]
    positions = lax.axis_index("kv") * span_len + jnp.arange(span_len, dtype=jnp.int32)
    new_slot = positions[None, :] == lengths[:, None]
    before = positions[None, :] < lengths[:, None]
    visible = positions[None, :] <= lengths[:, None]
    score_scale = HEAD_DIM ** (-0.5)
    keys_four = cache_keys.reshape(seq_count, span_len, heads_loc, 2, HEAD_DIM)
    scores = (
        jnp.einsum("bhcd,bphcd->bhcp", queries, keys_four, preferred_element_type=jnp.float32)
        * score_scale
    )
    new_score = (
        jnp.einsum("bhcd,bhcd->bhc", queries, key_new, preferred_element_type=jnp.float32)
        * score_scale
    )
    scores = jnp.where(new_slot[:, None, None, :], new_score[..., None], scores)
    visible_four = visible[:, None, None, :]
    block_max = jnp.max(jnp.where(visible_four, scores, -1e30), axis=-1)
    weights = jnp.where(visible_four, jnp.exp(scores - block_max[..., None]), 0.0)
    block_sum = jnp.sum(weights, axis=-1)
    weights_low = weights.astype(jnp.bfloat16)
    cache_weights = jnp.where(before[:, None, None, :], weights_low, jnp.zeros((), jnp.bfloat16))
    values_four = cache_values.reshape(seq_count, span_len, heads_loc, VALUE_DIM)
    block_out = jnp.einsum(
        "bhcp,bphe->bhce", cache_weights, values_four, preferred_element_type=jnp.float32
    )
    weight_new = jnp.sum(
        jnp.where(new_slot[:, None, None, :], weights_low.astype(jnp.float32), 0.0), axis=-1
    )
    block_out = block_out + weight_new[..., None] * value_new.astype(jnp.float32)[:, :, None, :]
    row_max, weight_total, combined = merged((block_max, block_sum, block_out), "kv", fold_maps)
    map_out = combined / weight_total[..., None]
    difference = map_out[:, :, 0] - lambda_head[None, :, None] * map_out[:, :, 1]
    inv_head = lax.rsqrt(jnp.mean(difference * difference, axis=-1, keepdims=True) + 1e-05)
    attended = (
        (difference * inv_head * head_gain)
        .astype(jnp.bfloat16)
        .reshape(seq_count, heads_loc * VALUE_DIM)
    )
    log_sums = row_max + jnp.log(weight_total)
    partial_value = jnp.dot(attended, out_weight, preferred_element_type=jnp.float32)
    layer_out = lax.psum_scatter(
        partial_value.astype(jnp.bfloat16), "tp", scatter_dimension=1, tiled=True
    )
    return (layer_out, log_sums)


MESH = pl.DeviceIdType.MESH
LANES = 128
ROWS = 8


STEPS = 32767.0
MASS_LANE = 64


def stat_lanes(groups, heads):
    return groups * (2 * heads + 1)


def fused_kernel(
    n_kv,
    n_tp,
    tok_hbm,
    gain_hbm,
    wq_hbm,
    wk_hbm,
    wv_hbm,
    lam_hbm,
    hgain_hbm,
    wo_hbm,
    ck_hbm,
    cv_hbm,
    len_hbm,
    out_ref,
    log_ref,
    tok_buf,
    gain_buf,
    lam_ref,
    hgain_ref,
    len_ref,
    wq_buf,
    wk_buf,
    wv_buf,
    k_buf,
    v_buf,
    wo_buf,
    q_buf,
    q_stat,
    q_scale,
    q_rot,
    new_buf,
    new_stat,
    att_buf,
    att_stat,
    head_buf,
    log_buf,
    o_send,
    o_recv,
    own_sem,
    w_sem,
    kv_sem,
    wo_sem,
    tok_ss,
    tok_rs,
    q_ss,
    q_rs,
    qs_ss,
    qs_rs,
    new_ss,
    new_rs,
    ns_ss,
    ns_rs,
    att_ss,
    att_rs,
    as_ss,
    as_rs,
    head_ss,
    head_rs,
    log_ss,
    log_rs,
    o_ss,
    o_rs,
    plane_sem,
    all_sem,
):
    f32, bf16, i32, i16 = jnp.float32, jnp.bfloat16, jnp.int32, jnp.int16
    my_kv, my_tp = lax.axis_index("kv"), lax.axis_index("tp")
    seqs, tok_w = tok_hbm.shape
    span = ck_hbm.shape[1]
    vdim = VALUE_DIM
    heads = n_kv
    per_owner = heads // 2
    groups = seqs // ROWS
    out_w = out_ref.shape[1]
    first_owner = n_kv // 2 - 1
    low_side = my_kv <= first_owner
    is_owner = (my_kv == first_owner) | (my_kv == first_owner + 1)
    far_owner = jnp.where(low_side, 1, 0)
    stride = 2 * heads + 1

    def tp_at(offset):
        return lax.rem(my_tp + offset, n_tp)

    def kv_at(offset):
        return lax.rem(my_kv + offset, n_kv)

    def kv_peer(t):
        down = n_kv - 1 - t
        down = jnp.where(down <= my_kv, down - 1, down)
        up = jnp.where(t >= my_kv, t + 1, t)
        return jnp.where(low_side, down, up)

    def slot_head(i, far):
        owner = far if i % 2 == 0 else 1 - far
        return owner * per_owner + i // 2

    def remote(src, dst, ss, rs, axis, peer):
        return pltpu.make_async_remote_copy(
            src_ref=src, dst_ref=dst, send_sem=ss, recv_sem=rs, device_id={axis: peer}, device_id_type=MESH
        )

    def send(*args):
        copy = remote(*args)
        copy.start()
        return copy

    def load(src, dst, sem):
        copy = pltpu.make_async_copy(src, dst, sem)
        copy.start()
        return copy

    barrier = pltpu.get_barrier_semaphore()
    gate, leader = n_tp - 1, n_tp - 2
    is_gate = my_tp == gate

    def signal(sem, axis, peer):
        pl.semaphore_signal(sem, inc=1, device_id={axis: peer}, device_id_type=MESH)

    for t in range(n_tp):
        if t != gate:

            @pl.when(my_tp != t)
            def _(t=t):
                signal(barrier, "tp", t)

    tok_load = load(tok_hbm, tok_buf.at[my_tp], own_sem.at[0])
    gain_load = load(gain_hbm, gain_buf.at[my_tp], own_sem.at[1])
    len_load = load(len_hbm, len_ref, own_sem.at[2])
    lam_load = load(lam_hbm, lam_ref, own_sem.at[3])
    hgain_load = load(hgain_hbm, hgain_ref, own_sem.at[4])
    tok_load.wait()
    gain_load.wait()
    w_loads = [
        load(w, buf, w_sem.at[m])
        for m, (w, buf) in enumerate(((wq_hbm, wq_buf), (wk_hbm, wk_buf), (wv_hbm, wv_buf)))
    ]
    kv_loads = []
    for i in range(heads):
        cols = pl.ds(pl.multiple_of(slot_head(i, far_owner) * vdim, vdim), vdim)
        kv_loads.append(
            (
                load(ck_hbm.at[:, :, cols], k_buf.at[i], kv_sem.at[2 * i]),
                load(cv_hbm.at[:, :, cols], v_buf.at[i], kv_sem.at[2 * i + 1]),
            )
        )
    wo_loads = []
    for i in range(n_tp):
        cols = pl.ds(pl.multiple_of(tp_at(i + 1) * out_w, out_w), out_w)
        wo_loads.append(load(wo_hbm.at[:, cols], wo_buf.at[i], wo_sem.at[i]))


    @pl.when(jnp.logical_not(is_gate))
    def _():
        pl.semaphore_wait(barrier, n_tp - 1)

    @pl.when(my_tp == leader)
    def _():
        signal(plane_sem, "tp", gate)

    @pl.when(is_gate)
    def _():
        pl.semaphore_wait(plane_sem, 1)
        for offset in range(1, n_kv):
            signal(barrier, "kv", kv_at(offset))

    sends = []
    tok_copies = []
    for o in range(n_tp - 1, 0, -1):
        peer = tp_at(o)
        for m, buf in enumerate((tok_buf, gain_buf)):
            tok_copies.append(
                send(
                    buf.at[my_tp],
                    buf.at[my_tp],
                    tok_ss.at[2 * o - 2 + m],
                    tok_rs.at[2 * o - 2 + m],
                    "tp",
                    peer,
                )
            )
    sends += tok_copies

    @pl.when(is_gate)
    def _():
        pl.semaphore_wait(barrier, n_kv - 1)
        for t in range(n_tp):
            if t != gate:
                signal(all_sem, "tp", t)

    len_load.wait()
    lane_id = lax.broadcasted_iota(i32, (seqs, LANES), 1)
    row_id = lax.broadcasted_iota(i32, (seqs, LANES), 0)
    lens = jnp.zeros((seqs, LANES), i32)
    for b in range(seqs):
        lens = jnp.where(row_id == b, len_ref[b], lens)
    half = HEAD_DIM // 2
    upper = lane_id >= half
    freq_id = jnp.where(upper, lane_id - half, lane_id).astype(f32)
    angles = lens.astype(f32) * jnp.exp(freq_id * (-2.0 * math.log(500000.0) / HEAD_DIM))
    cosine = jnp.cos(angles)
    sine = jnp.sin(angles)
    sine = jnp.where(upper, sine, -sine)

    def rotated(x):
        return (x * cosine + pltpu.roll(x, half, 1) * sine).astype(bf16)

    lane = lax.broadcasted_iota(i32, (ROWS, LANES), 1)

    def packed(columns):
        tile = jnp.zeros((ROWS, LANES), f32)
        for at, column in columns:
            tile = jnp.where(lane == at, column, tile)
        return tile

    def coded(x):
        top = jnp.maximum(jnp.max(jnp.abs(x), axis=1, keepdims=True), 1e-30)
        code = jnp.round(x * (STEPS / top)).astype(i32).astype(i16)
        return code, top * (1.0 / STEPS)

    def rows_of(g):
        return slice(g * ROWS, (g + 1) * ROWS)

    def decoded(codes, tile, width, at):
        value = codes.astype(i32).astype(f32)
        pieces = []
        for g in range(groups):
            rows = []
            for c in range(width):
                scale = tile[:, g * stride + at + c : g * stride + at + c + 1]
                rows.append(value[rows_of(g), c * LANES : (c + 1) * LANES] * scale)
            pieces.append(jnp.concatenate(rows, axis=1))
        return jnp.concatenate(pieces, axis=0)

    for copy in tok_copies:
        copy.wait_recv()
    squares = jnp.zeros((seqs, 1), f32)
    scaled_parts = []
    for s in range(n_tp):
        tok = tok_buf[s].astype(f32)
        squares = squares + jnp.sum(tok * tok, axis=1, keepdims=True)
        gain = gain_buf[s].astype(f32)
        gain = jnp.concatenate([gain[r : r + 1] for r in range(tok_w // LANES)], axis=1)
        scaled_parts.append((tok * gain).astype(bf16))
    scaled = jnp.concatenate(scaled_parts, axis=1)

    w_loads[0].wait()
    for j in range(per_owner):
        columns = [(g * stride + 2 * heads, squares[rows_of(g)]) for g in range(groups)]
        for h in (j, per_owner + j):
            part = jnp.dot(scaled, wq_buf[:, h * vdim : (h + 1) * vdim], preferred_element_type=f32)
            for c in range(2):
                cols = slice(c * HEAD_DIM, (c + 1) * HEAD_DIM)
                code, scale = coded(part[:, cols])
                q_buf[my_kv, h, :, cols] = code
                columns += [(g * stride + 2 * h + c, scale[rows_of(g)]) for g in range(groups)]
        q_stat[my_kv, j] = packed(columns)
        if j == 0:

            @pl.when(jnp.logical_not(is_gate))
            def _():
                pl.semaphore_wait(all_sem, 1)

        for t in range(n_kv - 1):
            at = q_stat.at[my_kv, j]
            sends.append(send(at, at, qs_ss.at[t, j], qs_rs.at[my_kv, j], "kv", kv_peer(t)))
        for i in (2 * j, 2 * j + 1):
            for t in range(n_kv - 1):
                peer = kv_peer(t)
                h = slot_head(i, jnp.where(peer <= first_owner, 1, 0))
                at = q_buf.at[my_kv, h]
                sends.append(send(at, at, q_ss.at[i, t], q_rs.at[my_kv, h], "kv", peer))

    columns = []
    w_loads[1].wait()
    w_loads[2].wait()
    for m, w in enumerate((wk_buf, wv_buf)):
        part = jnp.dot(scaled, w[...], preferred_element_type=f32)
        for j in range(2 * heads):
            code, scale = coded(part[:, j * HEAD_DIM : (j + 1) * HEAD_DIM])
            lo = m * vdim + (j % 2) * HEAD_DIM
            new_buf[my_kv, j // 2, :, lo : lo + HEAD_DIM] = code
            columns.append((m, j, scale))
    for m in range(2):
        new_stat[my_kv, m] = packed(
            [(g * stride + j, scale[rows_of(g)]) for mm, j, scale in columns if mm == m for g in range(groups)]
        )

    def new_copies(h):
        at = new_buf.at[my_kv, h]
        return remote(at, at, new_ss.at[h], new_rs.at[my_kv, h], "kv", first_owner + h // per_owner)

    def new_stat_copy(w):
        at = new_stat.at[my_kv]
        return remote(at, at, ns_ss.at[w], ns_rs.at[my_kv], "kv", first_owner + w)

    score_scale = HEAD_DIM ** (-0.5)
    wide = ROWS * span
    col = lax.broadcasted_iota(i32, (2 * ROWS, wide), 1)
    row = lax.broadcasted_iota(i32, (2 * ROWS, wide), 0)
    start = (row % ROWS) * span
    masks = []
    for g in range(groups):
        len_g = lens[rows_of(g), 0:1]
        len_g = jnp.concatenate([len_g, len_g], axis=0)
        limit = jnp.minimum(len_g - my_kv * span, span)
        masks.append((col >= start) & (col - start < limit))
    lane_q = lax.broadcasted_iota(i32, (ROWS, vdim), 1)
    contract_last = (((1,), (1,)), ((), ()))

    def att_copies(i):
        h = slot_head(i, far_owner)
        owner = first_owner + (far_owner if i % 2 == 0 else 1 - far_owner)
        at, stat_at = att_buf.at[my_kv, h], att_stat.at[my_kv, h]
        return [
            remote(at, at, att_ss.at[i], att_rs.at[my_kv, h], "kv", owner),
            remote(stat_at, stat_at, as_ss.at[i], as_rs.at[my_kv, h], "kv", owner),
        ]

    for j in range(per_owner):
        for o in range(1, n_kv):
            peer = kv_at(o)
            at = q_stat.at[peer, j]
            remote(at, at, qs_ss.at[o - 1, j], qs_rs.at[peer, j], "kv", peer).wait_recv()
        if j == 0:
            inv_rms = []
            for g in range(groups):
                at = g * stride + 2 * heads
                total = q_stat[0, 0][:, at : at + 1]
                for s in range(1, n_kv):
                    total = total + q_stat[s, 0][:, at : at + 1]
                inv_rms.append(lax.rsqrt(total / (tok_w * n_tp * n_kv) + 1e-06))
            inv_rms = jnp.concatenate(inv_rms, axis=0)
        for i in (2 * j, 2 * j + 1):
            h = slot_head(i, far_owner)
            for s in range(n_kv):
                tile = pltpu.roll(q_stat[s, j], lax.rem(LANES - 2 * h, LANES), 1)
                for c in range(2):
                    scale = jnp.concatenate([tile[:, g * stride + c : g * stride + c + 1] for g in range(groups)], axis=0)
                    cols = slice(c * HEAD_DIM, (c + 1) * HEAD_DIM)
                    q_scale[i, s, :, cols] = jnp.broadcast_to(scale * inv_rms, (seqs, HEAD_DIM))

    def arrived(i):
        h = slot_head(i, far_owner)
        for o in range(1, n_kv):
            peer = kv_at(o)
            at = q_buf.at[peer, h]
            remote(at, at, q_ss.at[i, o - 1], q_rs.at[peer, h], "kv", peer).wait_recv()
        kv_loads[i][0].wait()
        kv_loads[i][1].wait()

    def attend(slots):
        jobs = [(i, g) for i in slots for g in range(groups)]
        queries, scores, tops, weights, masses, outs = {}, {}, {}, {}, {}, {}
        for i in slots:
            h = slot_head(i, far_owner)
            total = jnp.zeros((seqs, vdim), f32)
            for s in range(n_kv):
                total = total + q_buf[s, h].astype(i32).astype(f32) * q_scale[i, s]
            maps = [rotated(total[:, c * HEAD_DIM : (c + 1) * HEAD_DIM]) for c in range(2)]
            for c in range(2):
                q_rot[i, :, c * HEAD_DIM : (c + 1) * HEAD_DIM] = maps[c]
            queries[i] = jnp.concatenate([m.astype(f32) for m in maps], axis=1)
        for i, g in jobs:
            q_g = queries[i][rows_of(g)]
            lhs = jnp.concatenate(
                [jnp.where(lane_q < HEAD_DIM, q_g, 0.0), jnp.where(lane_q < HEAD_DIM, 0.0, q_g)], axis=0
            ).astype(bf16)
            keys = k_buf[i, rows_of(g)].reshape(wide, vdim)
            scores[i, g] = lax.dot_general(lhs, keys, contract_last, preferred_element_type=f32)
        for i, g in jobs:
            scores[i, g] = jnp.where(masks[g], scores[i, g] * score_scale, -1e30)
            tops[i, g] = jnp.max(scores[i, g], axis=1, keepdims=True)
        for i, g in jobs:
            weights[i, g] = jnp.where(masks[g], jnp.exp(scores[i, g] - tops[i, g]), 0.0)
            masses[i, g] = jnp.sum(weights[i, g], axis=1, keepdims=True)
        for i, g in jobs:
            values = v_buf[i, rows_of(g)].reshape(wide, vdim)
            outs[i, g] = jnp.dot(weights[i, g].astype(bf16), values, preferred_element_type=f32)
        for i in slots:
            h = slot_head(i, far_owner)
            stats = []
            for g in range(groups):
                out = outs[i, g].astype(bf16)
                for c in range(2):
                    part = slice(c * ROWS, (c + 1) * ROWS)
                    att_buf[my_kv, h, c * seqs + g * ROWS : c * seqs + (g + 1) * ROWS] = out[part]
                    stats.append((2 * g + c, tops[i, g][part]))
                    stats.append((MASS_LANE + 2 * g + c, masses[i, g][part]))
            att_stat[my_kv, h] = packed(stats)

    def deliver(i):
        if i % 2 == 0:
            for copy in att_copies(i):
                copy.start()
        else:

            @pl.when(jnp.logical_not(is_owner))
            def _():
                for copy in att_copies(i):
                    copy.start()

    turns = [(i, i + 1) for i in range(0, heads - 2, 2)] + [(heads - 2,), (heads - 1,)]
    for j, turn in enumerate(turns):
        for i in turn:
            arrived(i)
        if j == 0:
            for w in range(2):

                @pl.when(my_kv != first_owner + w)
                def _(w=w):
                    new_stat_copy(w).start()
                    for k in range(per_owner):
                        new_copies(w * per_owner + k).start()

        attend(turn)
        for i in turn:
            deliver(i)

    lam_load.wait()
    hgain_load.wait()

    def head_copies(h):
        at, log_at = head_buf.at[h], log_buf.at[h]
        made = []
        for o in range(1, n_kv):
            peer = kv_at(o)
            made.append(remote(at, at, head_ss.at[h, o - 1], head_rs.at[h], "kv", peer))
        for o in range(1, n_kv):
            peer = kv_at(o)
            made.append(remote(log_at, log_at, log_ss.at[h, o - 1], log_rs.at[h], "kv", peer))
        return made

    def own_head(w, j):
        return w * per_owner + j

    for w in range(2):

        @pl.when(my_kv == first_owner + w)
        def _(w=w):
            for o in range(1, n_kv):
                peer = kv_at(o)
                at = new_stat.at[peer]
                remote(at, at, ns_ss.at[w], ns_rs.at[peer], "kv", peer).wait_recv()
            new_tiles, new_values = [], []
            for j in range(per_owner):
                h = own_head(w, j)
                for o in range(1, n_kv):
                    peer = kv_at(o)
                    at = new_buf.at[peer, h]
                    remote(at, at, new_ss.at[h], new_rs.at[peer, h], "kv", peer).wait_recv()
                k_sum = jnp.zeros((seqs, vdim), f32)
                v_sum = jnp.zeros((seqs, vdim), f32)
                for s in range(n_kv):
                    codes = new_buf[s, h]
                    k_sum = k_sum + decoded(codes[:, :vdim], new_stat[s, 0], 2, 2 * h)
                    v_sum = v_sum + decoded(codes[:, vdim:], new_stat[s, 1], 2, 2 * h)
                k_sum = k_sum * inv_rms
                new_values.append((v_sum * inv_rms).astype(bf16).astype(f32))
                scores = []
                for c in range(2):
                    cols = slice(c * HEAD_DIM, (c + 1) * HEAD_DIM)
                    k_new = rotated(k_sum[:, cols]).astype(f32)
                    score = jnp.sum(q_rot[2 * j + 1, :, cols].astype(f32) * k_new, axis=1, keepdims=True)
                    scores += [(2 * g + c, score[rows_of(g)] * score_scale) for g in range(groups)]
                new_tiles.append(packed(scores))
            for j in range(per_owner):
                h = own_head(w, j)
                for o in range(1, n_kv):
                    peer = kv_at(o)
                    at, stat_at = att_buf.at[peer, h], att_stat.at[peer, h]
                    remote(at, at, att_ss.at[0], att_rs.at[peer, h], "kv", peer).wait_recv()
                    remote(stat_at, stat_at, as_ss.at[0], as_rs.at[peer, h], "kv", peer).wait_recv()
                row_max = new_tiles[j]
                for s in range(n_kv):
                    row_max = jnp.maximum(row_max, att_stat[s, h])
                new_weight = jnp.exp(new_tiles[j] - row_max)
                total = new_weight
                scales = []
                for s in range(n_kv):
                    tile = att_stat[s, h]
                    scale = jnp.exp(tile - row_max)
                    total = total + scale * pltpu.roll(tile, LANES - MASS_LANE, 1)
                    scales.append(scale)
                share = 1.0 / total
                share = share * jnp.where(lane % 2 == 0, 1.0, -lam_ref[h])
                new_share = new_weight * share
                shares = [scale * share for scale in scales]
                log_buf[h] = row_max + jnp.log(total)
                pieces = []
                for g in range(groups):
                    at = 2 * g
                    piece = (new_share[:, at : at + 1] + new_share[:, at + 1 : at + 2]) * new_values[j][rows_of(g)]
                    for s in range(n_kv):
                        for c in range(2):
                            dst = slice(c * seqs + g * ROWS, c * seqs + (g + 1) * ROWS)
                            piece = piece + shares[s][:, at + c : at + c + 1] * att_buf[s, h, dst].astype(f32)
                    pieces.append(piece)
                difference = jnp.concatenate(pieces, axis=0)
                inv_head = lax.rsqrt(jnp.mean(difference * difference, axis=1, keepdims=True) + 1e-05)
                head_buf[h] = (difference * inv_head * hgain_ref[...]).astype(bf16)
                for copy in head_copies(h):
                    copy.start()

    for copy in wo_loads:
        copy.wait()
    head_order = [w * per_owner + j for j in range(per_owner) for w in range(2)]
    parts = [None] * n_tp
    for h in head_order:

        @pl.when(my_kv != first_owner + h // per_owner)
        def _(h=h):
            at = head_buf.at[h]
            remote(at, at, head_ss.at[h, 0], head_rs.at[h], "kv", kv_at(1)).wait_recv()

        attended = head_buf[h]
        for i in range(n_tp):
            term = jnp.dot(attended, wo_buf[i, h * vdim : (h + 1) * vdim], preferred_element_type=f32)
            parts[i] = term if parts[i] is None else parts[i] + term
    o_copies = []
    for i in range(n_tp - 1):
        o_send[i] = parts[i].astype(bf16)
        o_copies.append(send(o_send.at[i], o_recv.at[i], o_ss.at[i], o_rs.at[i], "tp", tp_at(i + 1)))
    sends += o_copies

    for h in range(heads):

        @pl.when(my_kv != first_owner + h // per_owner)
        def _(h=h):
            at = log_buf.at[h]
            remote(at, at, log_ss.at[h, 0], log_rs.at[h], "kv", kv_at(1)).wait_recv()

    pieces = []
    for g in range(groups):
        piece = jnp.zeros((ROWS, LANES), f32)
        for h in range(heads):
            tile = pltpu.roll(log_buf[h], (2 * h - 2 * g) % LANES, 1)
            piece = jnp.where((lane // 2) == h, tile, piece)
        pieces.append(piece)
    logs = jnp.concatenate(pieces, axis=0).T
    for h in range(heads):
        log_ref[h] = logs[2 * h : 2 * h + 2]

    result = parts[n_tp - 1].astype(bf16).astype(f32)
    for i, copy in enumerate(o_copies):
        copy.wait_recv()
        result = result + o_recv[i].astype(f32)
    out_ref[...] = result.astype(bf16)

    for copy in sends:
        copy.wait_send()
    for i in range(heads):
        if i % 2 == 0:
            for copy in att_copies(i):
                copy.wait_send()
        else:

            @pl.when(jnp.logical_not(is_owner))
            def _(i=i):
                for copy in att_copies(i):
                    copy.wait_send()

    for w in range(2):

        @pl.when(my_kv != first_owner + w)
        def _(w=w):
            new_stat_copy(w).wait_send()
            for j in range(per_owner):
                new_copies(w * per_owner + j).wait_send()

        @pl.when(my_kv == first_owner + w)
        def _(w=w):
            for j in range(per_owner):
                for copy in head_copies(own_head(w, j)):
                    copy.wait_send()


def hand_out(layer_in, logs_in, layer_out, logs_out):
    layer_out[...] = layer_in[...]
    logs_out[...] = logs_in[...]


def fused(
    n_kv,
    n_tp,
    tokens,
    norm_gain,
    query_weight,
    key_weight,
    value_weight,
    lambda_head,
    head_gain,
    out_weight,
    cache_keys,
    cache_values,
    lengths,
):
    seqs, tok_w = tokens.shape
    span = cache_keys.shape[1]
    depth, width = query_weight.shape
    heads = lambda_head.shape[0]
    out_w = out_weight.shape[1] // n_tp
    bf16, f32, i16 = jnp.bfloat16, jnp.float32, jnp.int16
    dma = pltpu.SemaphoreType.DMA
    anyspace = pl.BlockSpec(memory_space=pl.ANY)
    vmem = pl.BlockSpec(memory_space=pltpu.VMEM)
    k1, t1 = n_kv - 1, n_tp - 1
    operands = [
        pltpu.with_memory_space_constraint(a, pltpu.HBM)
        for a in (
            tokens,
            norm_gain.reshape(tok_w // LANES, LANES),
            query_weight,
            key_weight,
            value_weight,
            lambda_head,
            head_gain.reshape(1, VALUE_DIM),
            out_weight,
            cache_keys,
            cache_values,
            lengths,
        )
    ]
    layer, logs = pl.pallas_call(
        functools.partial(fused_kernel, n_kv, n_tp),
        out_shape=(pltpu.VMEM((seqs, out_w), bf16), pltpu.VMEM((heads, 2, seqs), f32)),
        in_specs=[anyspace] * len(operands),
        out_specs=(vmem, vmem),
        scratch_shapes=[
            pltpu.VMEM((n_tp, seqs, tok_w), bf16),
            pltpu.VMEM((n_tp, tok_w // LANES, LANES), bf16),
            pltpu.SMEM(lambda_head.shape, f32),
            pltpu.VMEM((1, VALUE_DIM), f32),
            pltpu.SMEM(lengths.shape, jnp.int32),
            pltpu.VMEM((depth, width), bf16),
            pltpu.VMEM((depth, width), bf16),
            pltpu.VMEM((depth, width), bf16),
            pltpu.VMEM((heads, seqs, span, VALUE_DIM), bf16),
            pltpu.VMEM((heads, seqs, span, VALUE_DIM), bf16),
            pltpu.VMEM((n_tp, out_weight.shape[0], out_w), bf16),
            pltpu.VMEM((n_kv, heads, seqs, VALUE_DIM), i16),
            pltpu.VMEM((n_kv, heads // 2, ROWS, LANES), f32),
            pltpu.VMEM((heads, n_kv, seqs, VALUE_DIM), f32),
            pltpu.VMEM((heads, seqs, VALUE_DIM), bf16),
            pltpu.VMEM((n_kv, heads, seqs, 2 * VALUE_DIM), i16),
            pltpu.VMEM((n_kv, 2, ROWS, LANES), f32),
            pltpu.VMEM((n_kv, heads, 2 * seqs, VALUE_DIM), bf16),
            pltpu.VMEM((n_kv, heads, ROWS, LANES), f32),
            pltpu.VMEM((heads, seqs, VALUE_DIM), bf16),
            pltpu.VMEM((heads, ROWS, LANES), f32),
            pltpu.VMEM((t1, seqs, out_w), bf16),
            pltpu.VMEM((t1, seqs, out_w), bf16),
            dma((5,)),
            dma((3,)),
            dma((2 * heads,)),
            dma((n_tp,)),
            dma((2 * t1,)),
            dma((2 * t1,)),
            dma((heads, k1)),
            dma((n_kv, heads)),
            dma((k1, heads // 2)),
            dma((n_kv, heads // 2)),
            dma((heads,)),
            dma((n_kv, heads)),
            dma((2,)),
            dma((n_kv,)),
            dma((heads,)),
            dma((n_kv, heads)),
            dma((heads,)),
            dma((n_kv, heads)),
            dma((heads, k1)),
            dma((heads,)),
            dma((heads, k1)),
            dma((heads,)),
            dma((t1,)),
            dma((t1,)),
            pltpu.SemaphoreType.REGULAR,
            pltpu.SemaphoreType.REGULAR,
        ],
        compiler_params=pltpu.CompilerParams(
            collective_id=0, has_side_effects=True, vmem_limit_bytes=40 * 1024 * 1024
        ),
        name="decode_step",
    )(*operands)
    layer, logs = (pltpu.with_memory_space_constraint(a, pltpu.VMEM) for a in (layer, logs))
    layer, logs = pl.pallas_call(
        hand_out,
        out_shape=(
            jax.ShapeDtypeStruct((seqs, out_w), bf16),
            jax.ShapeDtypeStruct((heads, 2, seqs), f32),
        ),
        in_specs=(vmem, vmem),
        out_specs=(vmem, vmem),
        name="hand_out",
    )(layer, logs)
    return layer, logs.transpose(2, 0, 1)


def fits_fused(n_kv, n_tp, tokens, lambda_head, out_weight, cache_keys):
    seqs, tok_w = tokens.shape
    heads = lambda_head.shape[0]
    resident = 2 * (4 * out_weight.size + 2 * cache_keys.size)
    groups = seqs // ROWS
    return (
        heads == n_kv
        and n_kv > 2
        and n_kv % 2 == 0
        and n_tp > 1
        and seqs % ROWS == 0
        and tok_w % LANES == 0
        and (out_weight.shape[1] // n_tp) % LANES == 0
        and groups * (2 * heads + 1) <= LANES
        and 2 * groups <= MASS_LANE
        and cache_keys.shape[1] % 16 == 0
        and resident <= 24 * 1024 * 1024
    )


def step(*args):
    n_kv, n_tp = lax.axis_size("kv"), lax.axis_size("tp")
    tokens, lambda_head, out_weight, cache_keys = args[0], args[5], args[7], args[8]
    if fits_fused(n_kv, n_tp, tokens, lambda_head, out_weight, cache_keys):
        return fused(n_kv, n_tp, *args)
    return on_device(*args)


def solution(mesh):
    in_specs = (
        P("grp", ("kv", "tp")),
        P(("kv", "tp")),
        P("kv", "tp"),
        P("kv", "tp"),
        P("kv", "tp"),
        P("tp"),
        P(),
        P("tp", "kv"),
        P("grp", "kv", "tp"),
        P("grp", "kv", "tp"),
        P("grp"),
    )
    out_specs = (P("grp", ("kv", "tp")), P("grp", "tp", None))
    return jax.shard_map(
        step, mesh=mesh, in_specs=in_specs, out_specs=out_specs, check_vma=False
    )
```

```python
import functools
import math

import jax
import jax.numpy as jnp
from jax import lax
from jax.experimental import pallas as pl
from jax.experimental.pallas import tpu as pltpu
from jax.sharding import PartitionSpec as P

D = 4096
HEAD_DIM = 128
VALUE_DIM = 256


def merged(part, axis, combine):
    gathered = jax.tree.map(lambda a: lax.all_gather(a, axis), part)

    def take(source):
        return jax.tree.map(lambda a: lax.dynamic_index_in_dim(a, source, 0, False), gathered)

    return lax.fori_loop(
        1, lax.axis_size(axis), lambda source, state: combine(state, take(source)), take(0)
    )


def rotate(vectors, lengths):
    half_dim = vectors.shape[-1] // 2
    freqs = jnp.power(
        jnp.float32(500000.0), -(jnp.arange(half_dim, dtype=jnp.float32) * 2.0 / vectors.shape[-1])
    )
    angles = lengths.astype(jnp.float32)[:, None] * freqs[None, :]
    cosine = jnp.cos(angles)[:, None, None, :]
    sine = jnp.sin(angles)[:, None, None, :]
    lower = vectors[..., :half_dim]
    upper = vectors[..., half_dim:]
    return jnp.concatenate([lower * cosine - upper * sine, upper * cosine + lower * sine], axis=-1)


def fold_maps(left_part, right_part):
    left_max, left_sum, left_out = left_part
    right_max, right_sum, right_out = right_part
    joint = jnp.maximum(left_max, right_max)
    left_scale = jnp.exp(left_max - joint)
    right_scale = jnp.exp(right_max - joint)
    return (
        joint,
        left_sum * left_scale + right_sum * right_scale,
        left_out * left_scale[..., None] + right_out * right_scale[..., None],
    )


def on_device(
    tokens,
    norm_gain,
    query_weight,
    key_weight,
    value_weight,
    lambda_head,
    head_gain,
    out_weight,
    cache_keys,
    cache_values,
    lengths,
):
    seq_count = tokens.shape[0]
    heads_loc = lambda_head.shape[0]
    token_block, gain_block = (
        lax.all_gather(tokens, "tp", axis=1, tiled=True),
        lax.all_gather(norm_gain, "tp", axis=0, tiled=True),
    )
    tok_float = token_block.astype(jnp.float32)
    scaled = (tok_float * gain_block.astype(jnp.float32)).astype(jnp.bfloat16)
    query_part = jnp.dot(scaled, query_weight, preferred_element_type=jnp.float32)
    key_part = jnp.dot(scaled, key_weight, preferred_element_type=jnp.float32)
    value_part = jnp.dot(scaled, value_weight, preferred_element_type=jnp.float32)
    local_squares = jnp.sum(tok_float * tok_float, axis=1)
    query_sum, key_sum, value_sum, row_squares = lax.psum(
        (query_part, key_part, value_part, local_squares), "kv"
    )
    inv_rms = lax.rsqrt(row_squares / D + 1e-06)[:, None]
    queries = rotate(
        (query_sum * inv_rms).reshape(seq_count, heads_loc, 2, HEAD_DIM), lengths
    ).astype(jnp.bfloat16)
    key_new = rotate(
        (key_sum * inv_rms).reshape(seq_count, heads_loc, 2, HEAD_DIM), lengths
    ).astype(jnp.bfloat16)
    value_new = (value_sum * inv_rms).astype(jnp.bfloat16).reshape(seq_count, heads_loc, VALUE_DIM)
    span_len = cache_keys.shape[1]
    positions = lax.axis_index("kv") * span_len + jnp.arange(span_len, dtype=jnp.int32)
    new_slot = positions[None, :] == lengths[:, None]
    before = positions[None, :] < lengths[:, None]
    visible = positions[None, :] <= lengths[:, None]
    score_scale = HEAD_DIM ** (-0.5)
    keys_four = cache_keys.reshape(seq_count, span_len, heads_loc, 2, HEAD_DIM)
    scores = (
        jnp.einsum("bhcd,bphcd->bhcp", queries, keys_four, preferred_element_type=jnp.float32)
        * score_scale
    )
    new_score = (
        jnp.einsum("bhcd,bhcd->bhc", queries, key_new, preferred_element_type=jnp.float32)
        * score_scale
    )
    scores = jnp.where(new_slot[:, None, None, :], new_score[..., None], scores)
    visible_four = visible[:, None, None, :]
    block_max = jnp.max(jnp.where(visible_four, scores, -1e30), axis=-1)
    weights = jnp.where(visible_four, jnp.exp(scores - block_max[..., None]), 0.0)
    block_sum = jnp.sum(weights, axis=-1)
    weights_low = weights.astype(jnp.bfloat16)
    cache_weights = jnp.where(before[:, None, None, :], weights_low, jnp.zeros((), jnp.bfloat16))
    values_four = cache_values.reshape(seq_count, span_len, heads_loc, VALUE_DIM)
    block_out = jnp.einsum(
        "bhcp,bphe->bhce", cache_weights, values_four, preferred_element_type=jnp.float32
    )
    weight_new = jnp.sum(
        jnp.where(new_slot[:, None, None, :], weights_low.astype(jnp.float32), 0.0), axis=-1
    )
    block_out = block_out + weight_new[..., None] * value_new.astype(jnp.float32)[:, :, None, :]
    row_max, weight_total, combined = merged((block_max, block_sum, block_out), "kv", fold_maps)
    map_out = combined / weight_total[..., None]
    difference = map_out[:, :, 0] - lambda_head[None, :, None] * map_out[:, :, 1]
    inv_head = lax.rsqrt(jnp.mean(difference * difference, axis=-1, keepdims=True) + 1e-05)
    attended = (
        (difference * inv_head * head_gain)
        .astype(jnp.bfloat16)
        .reshape(seq_count, heads_loc * VALUE_DIM)
    )
    log_sums = row_max + jnp.log(weight_total)
    partial_value = jnp.dot(attended, out_weight, preferred_element_type=jnp.float32)
    layer_out = lax.psum_scatter(
        partial_value.astype(jnp.bfloat16), "tp", scatter_dimension=1, tiled=True
    )
    return (layer_out, log_sums)


MESH = pl.DeviceIdType.MESH
LANES = 128
ROWS = 8


STEPS = 32767.0
ROUND_UP = 1.0 + 2.0**-7
SQUARE_LANES = 3
MASS_LANE = 64


def fused_kernel(
    n_kv,
    n_tp,
    tok_hbm,
    gain_hbm,
    wq_hbm,
    wk_hbm,
    wv_hbm,
    lam_hbm,
    hgain_hbm,
    wo_hbm,
    ck_hbm,
    cv_hbm,
    len_hbm,
    out_ref,
    log_ref,
    tok_buf,
    gain_buf,
    lam_ref,
    hgain_ref,
    len_ref,
    wq_buf,
    wk_buf,
    wv_buf,
    k_buf,
    v_buf,
    wo_buf,
    q_buf,
    q_stat,
    q_scale,
    q_rot,
    new_buf,
    new_stat,
    att_buf,
    att_stat,
    head_buf,
    log_buf,
    o_send,
    o_recv,
    own_sem,
    w_sem,
    kv_sem,
    wo_sem,
    tok_ss,
    tok_rs,
    q_ss,
    q_rs,
    qs_ss,
    qs_rs,
    new_ss,
    new_rs,
    ns_ss,
    ns_rs,
    att_ss,
    att_rs,
    as_ss,
    as_rs,
    head_ss,
    head_rs,
    log_ss,
    log_rs,
    o_ss,
    o_rs,
    plane_sem,
    all_sem,
):
    f32, bf16, i32, i16 = jnp.float32, jnp.bfloat16, jnp.int32, jnp.int16
    my_kv, my_tp = lax.axis_index("kv"), lax.axis_index("tp")
    seqs, tok_w = tok_hbm.shape
    span = ck_hbm.shape[1]
    vdim = VALUE_DIM
    heads = n_kv
    per_owner = heads // 2
    groups = seqs // ROWS
    out_w = out_ref.shape[1]
    first_owner = n_kv // 2 - 1
    low_side = my_kv <= first_owner
    is_owner = (my_kv == first_owner) | (my_kv == first_owner + 1)
    far_owner = jnp.where(low_side, 1, 0)
    stride = 2 * heads + SQUARE_LANES
    new_stride = 4 * heads

    def tp_at(offset):
        return lax.rem(my_tp + offset, n_tp)

    def kv_at(offset):
        return lax.rem(my_kv + offset, n_kv)

    def kv_peer(t):
        down = n_kv - 1 - t
        down = jnp.where(down <= my_kv, down - 1, down)
        up = jnp.where(t >= my_kv, t + 1, t)
        return jnp.where(low_side, down, up)

    def slot_head(i, far):
        owner = far if i % 2 == 0 else 1 - far
        return owner * per_owner + i // 2

    def remote(src, dst, ss, rs, axis, peer):
        return pltpu.make_async_remote_copy(
            src_ref=src, dst_ref=dst, send_sem=ss, recv_sem=rs, device_id={axis: peer}, device_id_type=MESH
        )

    def send(*args):
        copy = remote(*args)
        copy.start()
        return copy

    def load(src, dst, sem):
        copy = pltpu.make_async_copy(src, dst, sem)
        copy.start()
        return copy

    barrier = pltpu.get_barrier_semaphore()
    gate, leader = n_tp - 1, n_tp - 2
    is_gate = my_tp == gate

    def signal(sem, axis, peer):
        pl.semaphore_signal(sem, inc=1, device_id={axis: peer}, device_id_type=MESH)

    for t in range(n_tp):
        if t != gate:

            @pl.when(my_tp != t)
            def _(t=t):
                signal(barrier, "tp", t)

    tok_load = load(tok_hbm, tok_buf.at[my_tp], own_sem.at[0])
    gain_load = load(gain_hbm, gain_buf.at[my_tp], own_sem.at[1])
    len_load = load(len_hbm, len_ref, own_sem.at[2])
    lam_load = load(lam_hbm, lam_ref, own_sem.at[3])
    hgain_load = load(hgain_hbm, hgain_ref, own_sem.at[4])
    tok_load.wait()
    gain_load.wait()
    w_loads = [
        load(w, buf, w_sem.at[m])
        for m, (w, buf) in enumerate(((wq_hbm, wq_buf), (wk_hbm, wk_buf), (wv_hbm, wv_buf)))
    ]
    kv_loads = []
    for i in range(heads):
        cols = pl.ds(pl.multiple_of(slot_head(i, far_owner) * vdim, vdim), vdim)
        kv_loads.append(
            (
                load(ck_hbm.at[:, :, cols], k_buf.at[i], kv_sem.at[2 * i]),
                load(cv_hbm.at[:, :, cols], v_buf.at[i], kv_sem.at[2 * i + 1]),
            )
        )
    wo_loads = []
    for i in range(n_tp):
        cols = pl.ds(pl.multiple_of(tp_at(i + 1) * out_w, out_w), out_w)
        wo_loads.append(load(wo_hbm.at[:, cols], wo_buf.at[i], wo_sem.at[i]))


    @pl.when(jnp.logical_not(is_gate))
    def _():
        pl.semaphore_wait(barrier, n_tp - 1)

    @pl.when(my_tp == leader)
    def _():
        signal(plane_sem, "tp", gate)

    @pl.when(is_gate)
    def _():
        pl.semaphore_wait(plane_sem, 1)
        for offset in range(1, n_kv):
            signal(barrier, "kv", kv_at(offset))

    sends = []
    tok_copies = []
    for o in range(n_tp - 1, 0, -1):
        peer = tp_at(o)
        for m, buf in enumerate((tok_buf, gain_buf)):
            tok_copies.append(
                send(
                    buf.at[my_tp],
                    buf.at[my_tp],
                    tok_ss.at[2 * o - 2 + m],
                    tok_rs.at[2 * o - 2 + m],
                    "tp",
                    peer,
                )
            )
    sends += tok_copies

    @pl.when(is_gate)
    def _():
        pl.semaphore_wait(barrier, n_kv - 1)
        for t in range(n_tp):
            if t != gate:
                signal(all_sem, "tp", t)

    len_load.wait()
    lane_id = lax.broadcasted_iota(i32, (seqs, LANES), 1)
    row_id = lax.broadcasted_iota(i32, (seqs, LANES), 0)
    lens = jnp.zeros((seqs, LANES), i32)
    for b in range(seqs):
        lens = jnp.where(row_id == b, len_ref[b], lens)
    half = HEAD_DIM // 2
    upper = lane_id >= half
    freq_id = jnp.where(upper, lane_id - half, lane_id).astype(f32)
    angles = lens.astype(f32) * jnp.exp(freq_id * (-2.0 * math.log(500000.0) / HEAD_DIM))
    cosine = jnp.cos(angles)
    sine = jnp.sin(angles)
    sine = jnp.where(upper, sine, -sine)

    def rotated(x):
        return (x * cosine + pltpu.roll(x, half, 1) * sine).astype(bf16)

    lane = lax.broadcasted_iota(i32, (ROWS, LANES), 1)

    def packed(columns):
        tile = jnp.zeros((ROWS, LANES), f32)
        for at, column in columns:
            tile = jnp.where(lane == at, column, tile)
        return tile

    def coded(x):
        top = jnp.maximum(jnp.max(jnp.abs(x), axis=1, keepdims=True), 1e-30)
        scale = (top * (ROUND_UP / STEPS)).astype(bf16).astype(f32)
        return jnp.round(x * (1.0 / scale)).astype(i32).astype(i16), scale

    def thirds(x):
        high = x.astype(bf16).astype(f32)
        middle = (x - high).astype(bf16).astype(f32)
        return high, middle, x - high - middle

    def rows_of(g):
        return slice(g * ROWS, (g + 1) * ROWS)

    def decoded(codes, tile, width, at):
        value = codes.astype(i32).astype(f32)
        pieces = []
        for g in range(groups):
            rows = []
            for c in range(width):
                scale = tile[:, g * new_stride + at + c : g * new_stride + at + c + 1]
                rows.append(value[rows_of(g), c * LANES : (c + 1) * LANES] * scale)
            pieces.append(jnp.concatenate(rows, axis=1))
        return jnp.concatenate(pieces, axis=0)

    for copy in tok_copies:
        copy.wait_recv()
    squares = jnp.zeros((seqs, 1), f32)
    scaled_parts = []
    for s in range(n_tp):
        tok = tok_buf[s].astype(f32)
        squares = squares + jnp.sum(tok * tok, axis=1, keepdims=True)
        gain = gain_buf[s].astype(f32)
        gain = jnp.concatenate([gain[r : r + 1] for r in range(tok_w // LANES)], axis=1)
        scaled_parts.append((tok * gain).astype(bf16))
    scaled = jnp.concatenate(scaled_parts, axis=1)

    w_loads[0].wait()
    square_parts = thirds(squares)
    for j in range(per_owner):
        columns = [
            (g * stride + 2 * heads + m, third[rows_of(g)]) for m, third in enumerate(square_parts) for g in range(groups)
        ]
        for h in (j, per_owner + j):
            part = jnp.dot(scaled, wq_buf[:, h * vdim : (h + 1) * vdim], preferred_element_type=f32)
            for c in range(2):
                cols = slice(c * HEAD_DIM, (c + 1) * HEAD_DIM)
                code, scale = coded(part[:, cols])
                q_buf[my_kv, h, :, cols] = code
                columns += [(g * stride + 2 * h + c, scale[rows_of(g)]) for g in range(groups)]
        q_stat[my_kv, j] = packed(columns).astype(bf16)
        if j == 0:

            @pl.when(jnp.logical_not(is_gate))
            def _():
                pl.semaphore_wait(all_sem, 1)

        for t in range(n_kv - 1):
            at = q_stat.at[my_kv, j]
            sends.append(send(at, at, qs_ss.at[t, j], qs_rs.at[my_kv, j], "kv", kv_peer(t)))
        for i in (2 * j, 2 * j + 1):
            for t in range(n_kv - 1):
                peer = kv_peer(t)
                h = slot_head(i, jnp.where(peer <= first_owner, 1, 0))
                at = q_buf.at[my_kv, h]
                sends.append(send(at, at, q_ss.at[i, t], q_rs.at[my_kv, h], "kv", peer))

    columns = []
    w_loads[1].wait()
    w_loads[2].wait()
    for m, w in enumerate((wk_buf, wv_buf)):
        part = jnp.dot(scaled, w[...], preferred_element_type=f32)
        for j in range(2 * heads):
            code, scale = coded(part[:, j * HEAD_DIM : (j + 1) * HEAD_DIM])
            lo = m * vdim + (j % 2) * HEAD_DIM
            new_buf[my_kv, j // 2, :, lo : lo + HEAD_DIM] = code
            columns.append((m, j, scale))
    new_stat[my_kv] = packed(
        [(g * new_stride + 2 * heads * m + j, scale[rows_of(g)]) for m, j, scale in columns for g in range(groups)]
    ).astype(bf16)

    def new_copies(h):
        at = new_buf.at[my_kv, h]
        return remote(at, at, new_ss.at[h], new_rs.at[my_kv, h], "kv", first_owner + h // per_owner)

    def new_stat_copy(w):
        at = new_stat.at[my_kv]
        return remote(at, at, ns_ss.at[w], ns_rs.at[my_kv], "kv", first_owner + w)

    score_scale = HEAD_DIM ** (-0.5)
    wide = ROWS * span
    col = lax.broadcasted_iota(i32, (2 * ROWS, wide), 1)
    row = lax.broadcasted_iota(i32, (2 * ROWS, wide), 0)
    start = (row % ROWS) * span
    masks = []
    for g in range(groups):
        len_g = lens[rows_of(g), 0:1]
        len_g = jnp.concatenate([len_g, len_g], axis=0)
        limit = jnp.minimum(len_g - my_kv * span, span)
        masks.append((col >= start) & (col - start < limit))
    lane_q = lax.broadcasted_iota(i32, (ROWS, vdim), 1)
    contract_last = (((1,), (1,)), ((), ()))

    def att_copies(i):
        h = slot_head(i, far_owner)
        owner = first_owner + (far_owner if i % 2 == 0 else 1 - far_owner)
        at, stat_at = att_buf.at[my_kv, h], att_stat.at[my_kv, h]
        return [
            remote(at, at, att_ss.at[i], att_rs.at[my_kv, h], "kv", owner),
            remote(stat_at, stat_at, as_ss.at[i], as_rs.at[my_kv, h], "kv", owner),
        ]

    def stats_arrived(j):
        for o in range(1, n_kv):
            peer = kv_at(o)
            at = q_stat.at[peer, j]
            remote(at, at, qs_ss.at[o - 1, j], qs_rs.at[peer, j], "kv", peer).wait_recv()

    stats_arrived(0)
    inv_rms = []
    for g in range(groups):
        total = jnp.zeros((ROWS, 1), f32)
        for s in range(n_kv):
            tile = q_stat[s, 0].astype(f32)
            for m in range(SQUARE_LANES):
                at = g * stride + 2 * heads + m
                total = total + tile[:, at : at + 1]
        inv_rms.append(lax.rsqrt(total / (tok_w * n_tp * n_kv) + 1e-06))
    inv_rms = jnp.concatenate(inv_rms, axis=0)

    def spread_scales(j):
        for i in (2 * j, 2 * j + 1):
            h = slot_head(i, far_owner)
            for s in range(n_kv):
                tile = pltpu.roll(q_stat[s, j].astype(f32), lax.rem(LANES - 2 * h, LANES), 1)
                for c in range(2):
                    scale = jnp.concatenate([tile[:, g * stride + c : g * stride + c + 1] for g in range(groups)], axis=0)
                    cols = slice(c * HEAD_DIM, (c + 1) * HEAD_DIM)
                    q_scale[i, s, :, cols] = jnp.broadcast_to(scale * inv_rms, (seqs, HEAD_DIM))

    def arrived(i):
        h = slot_head(i, far_owner)
        for o in range(1, n_kv):
            peer = kv_at(o)
            at = q_buf.at[peer, h]
            remote(at, at, q_ss.at[i, o - 1], q_rs.at[peer, h], "kv", peer).wait_recv()
        kv_loads[i][0].wait()
        kv_loads[i][1].wait()

    def attend(slots):
        jobs = [(i, g) for i in slots for g in range(groups)]
        queries, scores, tops, weights, masses, outs = {}, {}, {}, {}, {}, {}
        for i in slots:
            h = slot_head(i, far_owner)
            total = jnp.zeros((seqs, vdim), f32)
            for s in range(n_kv):
                total = total + q_buf[s, h].astype(i32).astype(f32) * q_scale[i, s]
            maps = [rotated(total[:, c * HEAD_DIM : (c + 1) * HEAD_DIM]) for c in range(2)]
            for c in range(2):
                q_rot[i, :, c * HEAD_DIM : (c + 1) * HEAD_DIM] = maps[c]
            queries[i] = jnp.concatenate([m.astype(f32) for m in maps], axis=1)
        for i, g in jobs:
            q_g = queries[i][rows_of(g)]
            lhs = jnp.concatenate(
                [jnp.where(lane_q < HEAD_DIM, q_g, 0.0), jnp.where(lane_q < HEAD_DIM, 0.0, q_g)], axis=0
            ).astype(bf16)
            keys = k_buf[i, rows_of(g)].reshape(wide, vdim)
            scores[i, g] = lax.dot_general(lhs, keys, contract_last, preferred_element_type=f32)
        for i, g in jobs:
            scores[i, g] = jnp.where(masks[g], scores[i, g] * score_scale, -1e30)
            tops[i, g] = jnp.max(scores[i, g], axis=1, keepdims=True)
        for i, g in jobs:
            weights[i, g] = jnp.where(masks[g], jnp.exp(scores[i, g] - tops[i, g]), 0.0)
            masses[i, g] = jnp.sum(weights[i, g], axis=1, keepdims=True)
        for i, g in jobs:
            values = v_buf[i, rows_of(g)].reshape(wide, vdim)
            outs[i, g] = jnp.dot(weights[i, g].astype(bf16), values, preferred_element_type=f32)
        for i in slots:
            h = slot_head(i, far_owner)
            stats = []
            for g in range(groups):
                out = outs[i, g].astype(bf16)
                for c in range(2):
                    part = slice(c * ROWS, (c + 1) * ROWS)
                    att_buf[my_kv, h, c * seqs + g * ROWS : c * seqs + (g + 1) * ROWS] = out[part]
                    stats.append((2 * g + c, tops[i, g][part]))
                    stats.append((MASS_LANE + 2 * g + c, masses[i, g][part]))
            att_stat[my_kv, h] = packed(stats)

    def deliver(i):
        if i % 2 == 0:
            for copy in att_copies(i):
                copy.start()
        else:

            @pl.when(jnp.logical_not(is_owner))
            def _():
                for copy in att_copies(i):
                    copy.start()

    turns = [(i, i + 1) for i in range(0, heads - 2, 2)] + [(heads - 2,), (heads - 1,)]
    spread_scales(0)
    for j, turn in enumerate(turns):
        if turn[0] % 2 == 0 and turn[0] > 0:
            stats_arrived(turn[0] // 2)
            spread_scales(turn[0] // 2)
        for i in turn:
            arrived(i)
        if j == 0:
            for w in range(2):

                @pl.when(my_kv != first_owner + w)
                def _(w=w):
                    new_stat_copy(w).start()
                    for k in range(per_owner):
                        new_copies(w * per_owner + k).start()

        attend(turn)
        for i in turn:
            deliver(i)

    lam_load.wait()
    hgain_load.wait()

    def head_copies(h):
        at, log_at = head_buf.at[h], log_buf.at[h]
        made = []
        for o in range(1, n_kv):
            peer = kv_at(o)
            made.append(remote(at, at, head_ss.at[h, o - 1], head_rs.at[h], "kv", peer))
        for o in range(1, n_kv):
            peer = kv_at(o)
            made.append(remote(log_at, log_at, log_ss.at[h, o - 1], log_rs.at[h], "kv", peer))
        return made

    def own_head(w, j):
        return w * per_owner + j

    for w in range(2):

        @pl.when(my_kv == first_owner + w)
        def _(w=w):
            for o in range(1, n_kv):
                peer = kv_at(o)
                at = new_stat.at[peer]
                remote(at, at, ns_ss.at[w], ns_rs.at[peer], "kv", peer).wait_recv()
            new_tiles, new_values = [], []
            for j in range(per_owner):
                h = own_head(w, j)
                for o in range(1, n_kv):
                    peer = kv_at(o)
                    at = new_buf.at[peer, h]
                    remote(at, at, new_ss.at[h], new_rs.at[peer, h], "kv", peer).wait_recv()
                k_sum = jnp.zeros((seqs, vdim), f32)
                v_sum = jnp.zeros((seqs, vdim), f32)
                for s in range(n_kv):
                    codes = new_buf[s, h]
                    tile = new_stat[s].astype(f32)
                    k_sum = k_sum + decoded(codes[:, :vdim], tile, 2, 2 * h)
                    v_sum = v_sum + decoded(codes[:, vdim:], tile, 2, 2 * (heads + h))
                k_sum = k_sum * inv_rms
                new_values.append((v_sum * inv_rms).astype(bf16).astype(f32))
                scores = []
                for c in range(2):
                    cols = slice(c * HEAD_DIM, (c + 1) * HEAD_DIM)
                    k_new = rotated(k_sum[:, cols]).astype(f32)
                    score = jnp.sum(q_rot[2 * j + 1, :, cols].astype(f32) * k_new, axis=1, keepdims=True)
                    scores += [(2 * g + c, score[rows_of(g)] * score_scale) for g in range(groups)]
                new_tiles.append(packed(scores))
            for j in range(per_owner):
                h = own_head(w, j)
                for o in range(1, n_kv):
                    peer = kv_at(o)
                    at, stat_at = att_buf.at[peer, h], att_stat.at[peer, h]
                    remote(at, at, att_ss.at[0], att_rs.at[peer, h], "kv", peer).wait_recv()
                    remote(stat_at, stat_at, as_ss.at[0], as_rs.at[peer, h], "kv", peer).wait_recv()
                row_max = new_tiles[j]
                for s in range(n_kv):
                    row_max = jnp.maximum(row_max, att_stat[s, h])
                new_weight = jnp.exp(new_tiles[j] - row_max)
                total = new_weight
                scales = []
                for s in range(n_kv):
                    tile = att_stat[s, h]
                    scale = jnp.exp(tile - row_max)
                    total = total + scale * pltpu.roll(tile, LANES - MASS_LANE, 1)
                    scales.append(scale)
                share = 1.0 / total
                share = share * jnp.where(lane % 2 == 0, 1.0, -lam_ref[h])
                new_share = new_weight * share
                shares = [scale * share for scale in scales]
                log_buf[h] = row_max + jnp.log(total)
                pieces = []
                for g in range(groups):
                    at = 2 * g
                    piece = (new_share[:, at : at + 1] + new_share[:, at + 1 : at + 2]) * new_values[j][rows_of(g)]
                    for s in range(n_kv):
                        for c in range(2):
                            dst = slice(c * seqs + g * ROWS, c * seqs + (g + 1) * ROWS)
                            piece = piece + shares[s][:, at + c : at + c + 1] * att_buf[s, h, dst].astype(f32)
                    pieces.append(piece)
                difference = jnp.concatenate(pieces, axis=0)
                inv_head = lax.rsqrt(jnp.mean(difference * difference, axis=1, keepdims=True) + 1e-05)
                head_buf[h] = (difference * inv_head * hgain_ref[...]).astype(bf16)
                for copy in head_copies(h):
                    copy.start()

    for copy in wo_loads:
        copy.wait()
    head_order = [w * per_owner + j for j in range(per_owner) for w in range(2)]
    parts = [None] * n_tp
    for h in head_order:

        @pl.when(my_kv != first_owner + h // per_owner)
        def _(h=h):
            at = head_buf.at[h]
            remote(at, at, head_ss.at[h, 0], head_rs.at[h], "kv", kv_at(1)).wait_recv()

        attended = head_buf[h]
        for i in range(n_tp):
            term = jnp.dot(attended, wo_buf[i, h * vdim : (h + 1) * vdim], preferred_element_type=f32)
            parts[i] = term if parts[i] is None else parts[i] + term
    o_copies = []
    for i in range(n_tp - 1):
        o_send[i] = parts[i].astype(bf16)
        o_copies.append(send(o_send.at[i], o_recv.at[i], o_ss.at[i], o_rs.at[i], "tp", tp_at(i + 1)))
    sends += o_copies

    for h in range(heads):

        @pl.when(my_kv != first_owner + h // per_owner)
        def _(h=h):
            at = log_buf.at[h]
            remote(at, at, log_ss.at[h, 0], log_rs.at[h], "kv", kv_at(1)).wait_recv()

    pieces = []
    for g in range(groups):
        piece = jnp.zeros((ROWS, LANES), f32)
        for h in range(heads):
            tile = pltpu.roll(log_buf[h], (2 * h - 2 * g) % LANES, 1)
            piece = jnp.where((lane // 2) == h, tile, piece)
        pieces.append(piece)
    logs = jnp.concatenate(pieces, axis=0).T
    for h in range(heads):
        log_ref[h] = logs[2 * h : 2 * h + 2]

    result = parts[n_tp - 1].astype(bf16).astype(f32)
    for i, copy in enumerate(o_copies):
        copy.wait_recv()
        result = result + o_recv[i].astype(f32)
    out_ref[...] = result.astype(bf16)

    for copy in sends:
        copy.wait_send()
    for i in range(heads):
        if i % 2 == 0:
            for copy in att_copies(i):
                copy.wait_send()
        else:

            @pl.when(jnp.logical_not(is_owner))
            def _(i=i):
                for copy in att_copies(i):
                    copy.wait_send()

    for w in range(2):

        @pl.when(my_kv != first_owner + w)
        def _(w=w):
            new_stat_copy(w).wait_send()
            for j in range(per_owner):
                new_copies(w * per_owner + j).wait_send()

        @pl.when(my_kv == first_owner + w)
        def _(w=w):
            for j in range(per_owner):
                for copy in head_copies(own_head(w, j)):
                    copy.wait_send()


def hand_out(layer_in, logs_in, layer_out, logs_out):
    layer_out[...] = layer_in[...]
    logs_out[...] = logs_in[...]


def fused(
    n_kv,
    n_tp,
    tokens,
    norm_gain,
    query_weight,
    key_weight,
    value_weight,
    lambda_head,
    head_gain,
    out_weight,
    cache_keys,
    cache_values,
    lengths,
):
    seqs, tok_w = tokens.shape
    span = cache_keys.shape[1]
    depth, width = query_weight.shape
    heads = lambda_head.shape[0]
    out_w = out_weight.shape[1] // n_tp
    bf16, f32, i16 = jnp.bfloat16, jnp.float32, jnp.int16
    dma = pltpu.SemaphoreType.DMA
    anyspace = pl.BlockSpec(memory_space=pl.ANY)
    vmem = pl.BlockSpec(memory_space=pltpu.VMEM)
    k1, t1 = n_kv - 1, n_tp - 1
    operands = [
        pltpu.with_memory_space_constraint(a, pltpu.HBM)
        for a in (
            tokens,
            norm_gain.reshape(tok_w // LANES, LANES),
            query_weight,
            key_weight,
            value_weight,
            lambda_head,
            head_gain.reshape(1, VALUE_DIM),
            out_weight,
            cache_keys,
            cache_values,
            lengths,
        )
    ]
    layer, logs = pl.pallas_call(
        functools.partial(fused_kernel, n_kv, n_tp),
        out_shape=(pltpu.VMEM((seqs, out_w), bf16), pltpu.VMEM((heads, 2, seqs), f32)),
        in_specs=[anyspace] * len(operands),
        out_specs=(vmem, vmem),
        scratch_shapes=[
            pltpu.VMEM((n_tp, seqs, tok_w), bf16),
            pltpu.VMEM((n_tp, tok_w // LANES, LANES), bf16),
            pltpu.SMEM(lambda_head.shape, f32),
            pltpu.VMEM((1, VALUE_DIM), f32),
            pltpu.SMEM(lengths.shape, jnp.int32),
            pltpu.VMEM((depth, width), bf16),
            pltpu.VMEM((depth, width), bf16),
            pltpu.VMEM((depth, width), bf16),
            pltpu.VMEM((heads, seqs, span, VALUE_DIM), bf16),
            pltpu.VMEM((heads, seqs, span, VALUE_DIM), bf16),
            pltpu.VMEM((n_tp, out_weight.shape[0], out_w), bf16),
            pltpu.VMEM((n_kv, heads, seqs, VALUE_DIM), i16),
            pltpu.VMEM((n_kv, heads // 2, ROWS, LANES), bf16),
            pltpu.VMEM((heads, n_kv, seqs, VALUE_DIM), f32),
            pltpu.VMEM((heads, seqs, VALUE_DIM), bf16),
            pltpu.VMEM((n_kv, heads, seqs, 2 * VALUE_DIM), i16),
            pltpu.VMEM((n_kv, ROWS, LANES), bf16),
            pltpu.VMEM((n_kv, heads, 2 * seqs, VALUE_DIM), bf16),
            pltpu.VMEM((n_kv, heads, ROWS, LANES), f32),
            pltpu.VMEM((heads, seqs, VALUE_DIM), bf16),
            pltpu.VMEM((heads, ROWS, LANES), f32),
            pltpu.VMEM((t1, seqs, out_w), bf16),
            pltpu.VMEM((t1, seqs, out_w), bf16),
            dma((5,)),
            dma((3,)),
            dma((2 * heads,)),
            dma((n_tp,)),
            dma((2 * t1,)),
            dma((2 * t1,)),
            dma((heads, k1)),
            dma((n_kv, heads)),
            dma((k1, heads // 2)),
            dma((n_kv, heads // 2)),
            dma((heads,)),
            dma((n_kv, heads)),
            dma((2,)),
            dma((n_kv,)),
            dma((heads,)),
            dma((n_kv, heads)),
            dma((heads,)),
            dma((n_kv, heads)),
            dma((heads, k1)),
            dma((heads,)),
            dma((heads, k1)),
            dma((heads,)),
            dma((t1,)),
            dma((t1,)),
            pltpu.SemaphoreType.REGULAR,
            pltpu.SemaphoreType.REGULAR,
        ],
        compiler_params=pltpu.CompilerParams(
            collective_id=0, has_side_effects=True, vmem_limit_bytes=40 * 1024 * 1024
        ),
        name="decode_step",
    )(*operands)
    layer, logs = (pltpu.with_memory_space_constraint(a, pltpu.VMEM) for a in (layer, logs))
    layer, logs = pl.pallas_call(
        hand_out,
        out_shape=(
            jax.ShapeDtypeStruct((seqs, out_w), bf16),
            jax.ShapeDtypeStruct((heads, 2, seqs), f32),
        ),
        in_specs=(vmem, vmem),
        out_specs=(vmem, vmem),
        name="hand_out",
    )(layer, logs)
    return layer, logs.transpose(2, 0, 1)


def fits_fused(n_kv, n_tp, tokens, lambda_head, out_weight, cache_keys):
    seqs, tok_w = tokens.shape
    heads = lambda_head.shape[0]
    resident = 2 * (4 * out_weight.size + 2 * cache_keys.size)
    groups = seqs // ROWS
    return (
        heads == n_kv
        and n_kv > 2
        and n_kv % 2 == 0
        and n_tp > 1
        and seqs % ROWS == 0
        and tok_w % LANES == 0
        and (out_weight.shape[1] // n_tp) % LANES == 0
        and groups * max(2 * heads + SQUARE_LANES, 4 * heads) <= LANES
        and 2 * groups <= MASS_LANE
        and cache_keys.shape[1] % 16 == 0
        and resident <= 24 * 1024 * 1024
    )


def step(*args):
    n_kv, n_tp = lax.axis_size("kv"), lax.axis_size("tp")
    tokens, lambda_head, out_weight, cache_keys = args[0], args[5], args[7], args[8]
    if fits_fused(n_kv, n_tp, tokens, lambda_head, out_weight, cache_keys):
        return fused(n_kv, n_tp, *args)
    return on_device(*args)


def solution(mesh):
    in_specs = (
        P("grp", ("kv", "tp")),
        P(("kv", "tp")),
        P("kv", "tp"),
        P("kv", "tp"),
        P("kv", "tp"),
        P("tp"),
        P(),
        P("tp", "kv"),
        P("grp", "kv", "tp"),
        P("grp", "kv", "tp"),
        P("grp"),
    )
    out_specs = (P("grp", ("kv", "tp")), P("grp", "tp", None))
    return jax.shard_map(
        step, mesh=mesh, in_specs=in_specs, out_specs=out_specs, check_vma=False
    )
```

```python
import functools
import math

import jax
import jax.numpy as jnp
from jax import lax
from jax.experimental import pallas as pl
from jax.experimental.pallas import tpu as pltpu
from jax.sharding import PartitionSpec as P

D = 4096
HEAD_DIM = 128
VALUE_DIM = 256


def merged(part, axis, combine):
    gathered = jax.tree.map(lambda a: lax.all_gather(a, axis), part)

    def take(source):
        return jax.tree.map(lambda a: lax.dynamic_index_in_dim(a, source, 0, False), gathered)

    return lax.fori_loop(
        1, lax.axis_size(axis), lambda source, state: combine(state, take(source)), take(0)
    )


def rotate(vectors, lengths):
    half_dim = vectors.shape[-1] // 2
    freqs = jnp.power(
        jnp.float32(500000.0), -(jnp.arange(half_dim, dtype=jnp.float32) * 2.0 / vectors.shape[-1])
    )
    angles = lengths.astype(jnp.float32)[:, None] * freqs[None, :]
    cosine = jnp.cos(angles)[:, None, None, :]
    sine = jnp.sin(angles)[:, None, None, :]
    lower = vectors[..., :half_dim]
    upper = vectors[..., half_dim:]
    return jnp.concatenate([lower * cosine - upper * sine, upper * cosine + lower * sine], axis=-1)


def fold_maps(left_part, right_part):
    left_max, left_sum, left_out = left_part
    right_max, right_sum, right_out = right_part
    joint = jnp.maximum(left_max, right_max)
    left_scale = jnp.exp(left_max - joint)
    right_scale = jnp.exp(right_max - joint)
    return (
        joint,
        left_sum * left_scale + right_sum * right_scale,
        left_out * left_scale[..., None] + right_out * right_scale[..., None],
    )


def on_device(
    tokens,
    norm_gain,
    query_weight,
    key_weight,
    value_weight,
    lambda_head,
    head_gain,
    out_weight,
    cache_keys,
    cache_values,
    lengths,
):
    seq_count = tokens.shape[0]
    heads_loc = lambda_head.shape[0]
    token_block, gain_block = (
        lax.all_gather(tokens, "tp", axis=1, tiled=True),
        lax.all_gather(norm_gain, "tp", axis=0, tiled=True),
    )
    tok_float = token_block.astype(jnp.float32)
    scaled = (tok_float * gain_block.astype(jnp.float32)).astype(jnp.bfloat16)
    query_part = jnp.dot(scaled, query_weight, preferred_element_type=jnp.float32)
    key_part = jnp.dot(scaled, key_weight, preferred_element_type=jnp.float32)
    value_part = jnp.dot(scaled, value_weight, preferred_element_type=jnp.float32)
    local_squares = jnp.sum(tok_float * tok_float, axis=1)
    query_sum, key_sum, value_sum, row_squares = lax.psum(
        (query_part, key_part, value_part, local_squares), "kv"
    )
    inv_rms = lax.rsqrt(row_squares / D + 1e-06)[:, None]
    queries = rotate(
        (query_sum * inv_rms).reshape(seq_count, heads_loc, 2, HEAD_DIM), lengths
    ).astype(jnp.bfloat16)
    key_new = rotate(
        (key_sum * inv_rms).reshape(seq_count, heads_loc, 2, HEAD_DIM), lengths
    ).astype(jnp.bfloat16)
    value_new = (value_sum * inv_rms).astype(jnp.bfloat16).reshape(seq_count, heads_loc, VALUE_DIM)
    span_len = cache_keys.shape[1]
    positions = lax.axis_index("kv") * span_len + jnp.arange(span_len, dtype=jnp.int32)
    new_slot = positions[None, :] == lengths[:, None]
    before = positions[None, :] < lengths[:, None]
    visible = positions[None, :] <= lengths[:, None]
    score_scale = HEAD_DIM ** (-0.5)
    keys_four = cache_keys.reshape(seq_count, span_len, heads_loc, 2, HEAD_DIM)
    scores = (
        jnp.einsum("bhcd,bphcd->bhcp", queries, keys_four, preferred_element_type=jnp.float32)
        * score_scale
    )
    new_score = (
        jnp.einsum("bhcd,bhcd->bhc", queries, key_new, preferred_element_type=jnp.float32)
        * score_scale
    )
    scores = jnp.where(new_slot[:, None, None, :], new_score[..., None], scores)
    visible_four = visible[:, None, None, :]
    block_max = jnp.max(jnp.where(visible_four, scores, -1e30), axis=-1)
    weights = jnp.where(visible_four, jnp.exp(scores - block_max[..., None]), 0.0)
    block_sum = jnp.sum(weights, axis=-1)
    weights_low = weights.astype(jnp.bfloat16)
    cache_weights = jnp.where(before[:, None, None, :], weights_low, jnp.zeros((), jnp.bfloat16))
    values_four = cache_values.reshape(seq_count, span_len, heads_loc, VALUE_DIM)
    block_out = jnp.einsum(
        "bhcp,bphe->bhce", cache_weights, values_four, preferred_element_type=jnp.float32
    )
    weight_new = jnp.sum(
        jnp.where(new_slot[:, None, None, :], weights_low.astype(jnp.float32), 0.0), axis=-1
    )
    block_out = block_out + weight_new[..., None] * value_new.astype(jnp.float32)[:, :, None, :]
    row_max, weight_total, combined = merged((block_max, block_sum, block_out), "kv", fold_maps)
    map_out = combined / weight_total[..., None]
    difference = map_out[:, :, 0] - lambda_head[None, :, None] * map_out[:, :, 1]
    inv_head = lax.rsqrt(jnp.mean(difference * difference, axis=-1, keepdims=True) + 1e-05)
    attended = (
        (difference * inv_head * head_gain)
        .astype(jnp.bfloat16)
        .reshape(seq_count, heads_loc * VALUE_DIM)
    )
    log_sums = row_max + jnp.log(weight_total)
    partial_value = jnp.dot(attended, out_weight, preferred_element_type=jnp.float32)
    layer_out = lax.psum_scatter(
        partial_value.astype(jnp.bfloat16), "tp", scatter_dimension=1, tiled=True
    )
    return (layer_out, log_sums)


MESH = pl.DeviceIdType.MESH
LANES = 128
ROWS = 8


STEPS = 32767.0
ROUND_UP = 1.0 + 2.0**-7
SQUARE_LANES = 3
MASS_LANE = 64


def fused_kernel(
    n_kv,
    n_tp,
    tok_hbm,
    gain_hbm,
    wq_hbm,
    wk_hbm,
    wv_hbm,
    lam_hbm,
    hgain_hbm,
    wo_hbm,
    ck_hbm,
    cv_hbm,
    len_hbm,
    out_ref,
    log_ref,
    tok_buf,
    gain_buf,
    lam_ref,
    hgain_ref,
    len_ref,
    wq_buf,
    wk_buf,
    wv_buf,
    k_buf,
    v_buf,
    wo_buf,
    q_buf,
    q_stat,
    q_scale,
    q_rot,
    new_buf,
    new_stat,
    att_buf,
    att_stat,
    head_buf,
    log_buf,
    o_send,
    o_recv,
    own_sem,
    w_sem,
    kv_sem,
    wo_sem,
    tok_ss,
    tok_rs,
    q_ss,
    q_rs,
    qs_ss,
    qs_rs,
    new_ss,
    new_rs,
    ns_ss,
    ns_rs,
    att_ss,
    att_rs,
    as_ss,
    as_rs,
    head_ss,
    head_rs,
    log_ss,
    log_rs,
    o_ss,
    o_rs,
    plane_sem,
    all_sem,
):
    f32, bf16, i32, i16 = jnp.float32, jnp.bfloat16, jnp.int32, jnp.int16
    my_kv, my_tp = lax.axis_index("kv"), lax.axis_index("tp")
    seqs, tok_w = tok_hbm.shape
    span = ck_hbm.shape[1]
    vdim = VALUE_DIM
    heads = n_kv
    per_owner = heads // 2
    groups = seqs // ROWS
    out_w = out_ref.shape[1]
    first_owner = n_kv // 2 - 1
    low_side = my_kv <= first_owner
    is_owner = (my_kv == first_owner) | (my_kv == first_owner + 1)
    far_owner = jnp.where(low_side, 1, 0)
    stride = 2 * heads + SQUARE_LANES
    new_stride = 4 * heads

    def tp_at(offset):
        return lax.rem(my_tp + offset, n_tp)

    def kv_at(offset):
        return lax.rem(my_kv + offset, n_kv)

    def kv_peer(t):
        down = n_kv - 1 - t
        down = jnp.where(down <= my_kv, down - 1, down)
        up = jnp.where(t >= my_kv, t + 1, t)
        return jnp.where(low_side, down, up)

    def slot_head(i, far):
        owner = far if i < per_owner else 1 - far
        return owner * per_owner + i % per_owner

    def remote(src, dst, ss, rs, axis, peer):
        return pltpu.make_async_remote_copy(
            src_ref=src, dst_ref=dst, send_sem=ss, recv_sem=rs, device_id={axis: peer}, device_id_type=MESH
        )

    def send(*args):
        copy = remote(*args)
        copy.start()
        return copy

    def load(src, dst, sem):
        copy = pltpu.make_async_copy(src, dst, sem)
        copy.start()
        return copy

    barrier = pltpu.get_barrier_semaphore()
    gate, leader = n_tp - 1, n_tp - 2
    is_gate = my_tp == gate

    def signal(sem, axis, peer):
        pl.semaphore_signal(sem, inc=1, device_id={axis: peer}, device_id_type=MESH)

    for t in range(n_tp):
        if t != gate:

            @pl.when(my_tp != t)
            def _(t=t):
                signal(barrier, "tp", t)

    tok_load = load(tok_hbm, tok_buf.at[my_tp], own_sem.at[0])
    gain_load = load(gain_hbm, gain_buf.at[my_tp], own_sem.at[1])
    len_load = load(len_hbm, len_ref, own_sem.at[2])
    lam_load = load(lam_hbm, lam_ref, own_sem.at[3])
    hgain_load = load(hgain_hbm, hgain_ref, own_sem.at[4])
    tok_load.wait()
    gain_load.wait()
    w_loads = [
        load(w, buf, w_sem.at[m])
        for m, (w, buf) in enumerate(((wq_hbm, wq_buf), (wk_hbm, wk_buf), (wv_hbm, wv_buf)))
    ]
    kv_loads = []
    for i in range(heads):
        cols = pl.ds(pl.multiple_of(slot_head(i, far_owner) * vdim, vdim), vdim)
        kv_loads.append(
            (
                load(ck_hbm.at[:, :, cols], k_buf.at[i], kv_sem.at[2 * i]),
                load(cv_hbm.at[:, :, cols], v_buf.at[i], kv_sem.at[2 * i + 1]),
            )
        )
    wo_loads = []
    for i in range(n_tp):
        cols = pl.ds(pl.multiple_of(tp_at(i + 1) * out_w, out_w), out_w)
        wo_loads.append(load(wo_hbm.at[:, cols], wo_buf.at[i], wo_sem.at[i]))


    @pl.when(jnp.logical_not(is_gate))
    def _():
        pl.semaphore_wait(barrier, n_tp - 1)

    @pl.when(my_tp == leader)
    def _():
        signal(plane_sem, "tp", gate)

    @pl.when(is_gate)
    def _():
        pl.semaphore_wait(plane_sem, 1)
        for offset in range(1, n_kv):
            signal(barrier, "kv", kv_at(offset))

    sends = []
    tok_copies = []
    for o in range(n_tp - 1, 0, -1):
        peer = tp_at(o)
        for m, buf in enumerate((tok_buf, gain_buf)):
            tok_copies.append(
                send(
                    buf.at[my_tp],
                    buf.at[my_tp],
                    tok_ss.at[2 * o - 2 + m],
                    tok_rs.at[2 * o - 2 + m],
                    "tp",
                    peer,
                )
            )
    sends += tok_copies

    @pl.when(is_gate)
    def _():
        pl.semaphore_wait(barrier, n_kv - 1)
        for t in range(n_tp):
            if t != gate:
                signal(all_sem, "tp", t)

    len_load.wait()
    lane_id = lax.broadcasted_iota(i32, (seqs, LANES), 1)
    row_id = lax.broadcasted_iota(i32, (seqs, LANES), 0)
    lens = jnp.zeros((seqs, LANES), i32)
    for b in range(seqs):
        lens = jnp.where(row_id == b, len_ref[b], lens)
    half = HEAD_DIM // 2
    upper = lane_id >= half
    freq_id = jnp.where(upper, lane_id - half, lane_id).astype(f32)
    angles = lens.astype(f32) * jnp.exp(freq_id * (-2.0 * math.log(500000.0) / HEAD_DIM))
    cosine = jnp.cos(angles)
    sine = jnp.sin(angles)
    sine = jnp.where(upper, sine, -sine)

    def rotated(x):
        return (x * cosine + pltpu.roll(x, half, 1) * sine).astype(bf16)

    lane = lax.broadcasted_iota(i32, (ROWS, LANES), 1)

    def packed(columns):
        tile = jnp.zeros((ROWS, LANES), f32)
        for at, column in columns:
            tile = jnp.where(lane == at, column, tile)
        return tile

    def coded(x):
        top = jnp.maximum(jnp.max(jnp.abs(x), axis=1, keepdims=True), 1e-30)
        scale = (top * (ROUND_UP / STEPS)).astype(bf16).astype(f32)
        return jnp.round(x * (1.0 / scale)).astype(i32).astype(i16), scale

    def thirds(x):
        high = x.astype(bf16).astype(f32)
        middle = (x - high).astype(bf16).astype(f32)
        return high, middle, x - high - middle

    def rows_of(g):
        return slice(g * ROWS, (g + 1) * ROWS)

    def decoded(codes, tile, width, at):
        value = codes.astype(i32).astype(f32)
        pieces = []
        for g in range(groups):
            rows = []
            for c in range(width):
                scale = tile[:, g * new_stride + at + c : g * new_stride + at + c + 1]
                rows.append(value[rows_of(g), c * LANES : (c + 1) * LANES] * scale)
            pieces.append(jnp.concatenate(rows, axis=1))
        return jnp.concatenate(pieces, axis=0)

    for copy in tok_copies:
        copy.wait_recv()
    squares = jnp.zeros((seqs, 1), f32)
    scaled_parts = []
    for s in range(n_tp):
        tok = tok_buf[s].astype(f32)
        squares = squares + jnp.sum(tok * tok, axis=1, keepdims=True)
        gain = gain_buf[s].astype(f32)
        gain = jnp.concatenate([gain[r : r + 1] for r in range(tok_w // LANES)], axis=1)
        scaled_parts.append((tok * gain).astype(bf16))
    scaled = jnp.concatenate(scaled_parts, axis=1)

    w_loads[0].wait()
    square_parts = thirds(squares)
    columns = [
        (g * stride + 2 * heads + m, third[rows_of(g)]) for m, third in enumerate(square_parts) for g in range(groups)
    ]
    for h in range(heads):
        part = jnp.dot(scaled, wq_buf[:, h * vdim : (h + 1) * vdim], preferred_element_type=f32)
        for c in range(2):
            cols = slice(c * HEAD_DIM, (c + 1) * HEAD_DIM)
            code, scale = coded(part[:, cols])
            q_buf[my_kv, h, :, cols] = code
            columns += [(g * stride + 2 * h + c, scale[rows_of(g)]) for g in range(groups)]
    q_stat[my_kv] = packed(columns).astype(bf16)

    @pl.when(jnp.logical_not(is_gate))
    def _():
        pl.semaphore_wait(all_sem, 1)

    for t in range(n_kv - 1):
        at = q_stat.at[my_kv]
        sends.append(send(at, at, qs_ss.at[t], qs_rs.at[my_kv], "kv", kv_peer(t)))
    for i in range(heads):
        for t in range(n_kv - 1):
            peer = kv_peer(t)
            h = slot_head(i, jnp.where(peer <= first_owner, 1, 0))
            at = q_buf.at[my_kv, h]
            sends.append(send(at, at, q_ss.at[i, t], q_rs.at[my_kv, h], "kv", peer))

    columns = []
    w_loads[1].wait()
    w_loads[2].wait()
    for m, w in enumerate((wk_buf, wv_buf)):
        part = jnp.dot(scaled, w[...], preferred_element_type=f32)
        for j in range(2 * heads):
            code, scale = coded(part[:, j * HEAD_DIM : (j + 1) * HEAD_DIM])
            lo = m * vdim + (j % 2) * HEAD_DIM
            new_buf[my_kv, j // 2, :, lo : lo + HEAD_DIM] = code
            columns.append((m, j, scale))
    new_stat[my_kv] = packed(
        [(g * new_stride + 2 * heads * m + j, scale[rows_of(g)]) for m, j, scale in columns for g in range(groups)]
    ).astype(bf16)

    def new_copies(h):
        at = new_buf.at[my_kv, h]
        return remote(at, at, new_ss.at[h], new_rs.at[my_kv, h], "kv", first_owner + h // per_owner)

    def new_stat_copy(w):
        at = new_stat.at[my_kv]
        return remote(at, at, ns_ss.at[w], ns_rs.at[my_kv], "kv", first_owner + w)

    score_scale = HEAD_DIM ** (-0.5)
    wide = ROWS * span
    col = lax.broadcasted_iota(i32, (2 * ROWS, wide), 1)
    row = lax.broadcasted_iota(i32, (2 * ROWS, wide), 0)
    start = (row % ROWS) * span
    masks = []
    for g in range(groups):
        len_g = lens[rows_of(g), 0:1]
        len_g = jnp.concatenate([len_g, len_g], axis=0)
        limit = jnp.minimum(len_g - my_kv * span, span)
        masks.append((col >= start) & (col - start < limit))
    lane_q = lax.broadcasted_iota(i32, (ROWS, vdim), 1)
    contract_last = (((1,), (1,)), ((), ()))

    def att_copies(i):
        h = slot_head(i, far_owner)
        owner = first_owner + (far_owner if i < per_owner else 1 - far_owner)
        at, stat_at = att_buf.at[my_kv, h], att_stat.at[my_kv, h]
        return [
            remote(at, at, att_ss.at[i], att_rs.at[my_kv, h], "kv", owner),
            remote(stat_at, stat_at, as_ss.at[i], as_rs.at[my_kv, h], "kv", owner),
        ]

    for o in range(1, n_kv):
        peer = kv_at(o)
        at = q_stat.at[peer]
        remote(at, at, qs_ss.at[o - 1], qs_rs.at[peer], "kv", peer).wait_recv()
    inv_rms = []
    for g in range(groups):
        total = jnp.zeros((ROWS, 1), f32)
        for s in range(n_kv):
            tile = q_stat[s].astype(f32)
            for m in range(SQUARE_LANES):
                at = g * stride + 2 * heads + m
                total = total + tile[:, at : at + 1]
        inv_rms.append(lax.rsqrt(total / (tok_w * n_tp * n_kv) + 1e-06))
    inv_rms = jnp.concatenate(inv_rms, axis=0)

    def spread_scales(slots):
        for i in slots:
            h = slot_head(i, far_owner)
            for s in range(n_kv):
                tile = pltpu.roll(q_stat[s].astype(f32), lax.rem(LANES - 2 * h, LANES), 1)
                for c in range(2):
                    scale = jnp.concatenate([tile[:, g * stride + c : g * stride + c + 1] for g in range(groups)], axis=0)
                    cols = slice(c * HEAD_DIM, (c + 1) * HEAD_DIM)
                    q_scale[i, s, :, cols] = jnp.broadcast_to(scale * inv_rms, (seqs, HEAD_DIM))

    def arrived(i):
        h = slot_head(i, far_owner)
        for o in range(1, n_kv):
            peer = kv_at(o)
            at = q_buf.at[peer, h]
            remote(at, at, q_ss.at[i, o - 1], q_rs.at[peer, h], "kv", peer).wait_recv()
        kv_loads[i][0].wait()
        kv_loads[i][1].wait()

    def attend(slots):
        jobs = [(i, g) for i in slots for g in range(groups)]
        queries, scores, tops, weights, masses, outs = {}, {}, {}, {}, {}, {}
        for i in slots:
            h = slot_head(i, far_owner)
            total = jnp.zeros((seqs, vdim), f32)
            for s in range(n_kv):
                total = total + q_buf[s, h].astype(i32).astype(f32) * q_scale[i, s]
            maps = [rotated(total[:, c * HEAD_DIM : (c + 1) * HEAD_DIM]) for c in range(2)]
            for c in range(2):
                q_rot[i, :, c * HEAD_DIM : (c + 1) * HEAD_DIM] = maps[c]
            queries[i] = jnp.concatenate([m.astype(f32) for m in maps], axis=1)
        for i, g in jobs:
            q_g = queries[i][rows_of(g)]
            lhs = jnp.concatenate(
                [jnp.where(lane_q < HEAD_DIM, q_g, 0.0), jnp.where(lane_q < HEAD_DIM, 0.0, q_g)], axis=0
            ).astype(bf16)
            keys = k_buf[i, rows_of(g)].reshape(wide, vdim)
            scores[i, g] = lax.dot_general(lhs, keys, contract_last, preferred_element_type=f32)
        for i, g in jobs:
            scores[i, g] = jnp.where(masks[g], scores[i, g] * score_scale, -1e30)
            tops[i, g] = jnp.max(scores[i, g], axis=1, keepdims=True)
        for i, g in jobs:
            weights[i, g] = jnp.where(masks[g], jnp.exp(scores[i, g] - tops[i, g]), 0.0)
            masses[i, g] = jnp.sum(weights[i, g], axis=1, keepdims=True)
        for i, g in jobs:
            values = v_buf[i, rows_of(g)].reshape(wide, vdim)
            outs[i, g] = jnp.dot(weights[i, g].astype(bf16), values, preferred_element_type=f32)
        for i in slots:
            h = slot_head(i, far_owner)
            stats = []
            for g in range(groups):
                out = outs[i, g].astype(bf16)
                for c in range(2):
                    part = slice(c * ROWS, (c + 1) * ROWS)
                    att_buf[my_kv, h, c * seqs + g * ROWS : c * seqs + (g + 1) * ROWS] = out[part]
                    stats.append((2 * g + c, tops[i, g][part]))
                    stats.append((MASS_LANE + 2 * g + c, masses[i, g][part]))
            att_stat[my_kv, h] = packed(stats)

    def deliver(i):
        if i < per_owner:
            for copy in att_copies(i):
                copy.start()
        else:

            @pl.when(jnp.logical_not(is_owner))
            def _():
                for copy in att_copies(i):
                    copy.start()

    turns = [(i,) for i in range(heads)]
    spread_scales(range(heads))
    for j, turn in enumerate(turns):
        for i in turn:
            arrived(i)
        if j == 0:
            for w in range(2):

                @pl.when(my_kv != first_owner + w)
                def _(w=w):
                    new_stat_copy(w).start()
                    for k in range(per_owner):
                        new_copies(w * per_owner + k).start()

        attend(turn)
        for i in turn:
            deliver(i)

    lam_load.wait()
    hgain_load.wait()

    def head_copies(h):
        at, log_at = head_buf.at[h], log_buf.at[h]
        made = []
        for o in range(1, n_kv):
            peer = kv_at(o)
            made.append(remote(at, at, head_ss.at[h, o - 1], head_rs.at[h], "kv", peer))
        for o in range(1, n_kv):
            peer = kv_at(o)
            made.append(remote(log_at, log_at, log_ss.at[h, o - 1], log_rs.at[h], "kv", peer))
        return made

    def own_head(w, j):
        return w * per_owner + j

    for w in range(2):

        @pl.when(my_kv == first_owner + w)
        def _(w=w):
            for o in range(1, n_kv):
                peer = kv_at(o)
                at = new_stat.at[peer]
                remote(at, at, ns_ss.at[w], ns_rs.at[peer], "kv", peer).wait_recv()
            new_tiles, new_values = [], []
            for j in range(per_owner):
                h = own_head(w, j)
                for o in range(1, n_kv):
                    peer = kv_at(o)
                    at = new_buf.at[peer, h]
                    remote(at, at, new_ss.at[h], new_rs.at[peer, h], "kv", peer).wait_recv()
                k_sum = jnp.zeros((seqs, vdim), f32)
                v_sum = jnp.zeros((seqs, vdim), f32)
                for s in range(n_kv):
                    codes = new_buf[s, h]
                    tile = new_stat[s].astype(f32)
                    k_sum = k_sum + decoded(codes[:, :vdim], tile, 2, 2 * h)
                    v_sum = v_sum + decoded(codes[:, vdim:], tile, 2, 2 * (heads + h))
                k_sum = k_sum * inv_rms
                new_values.append((v_sum * inv_rms).astype(bf16).astype(f32))
                scores = []
                for c in range(2):
                    cols = slice(c * HEAD_DIM, (c + 1) * HEAD_DIM)
                    k_new = rotated(k_sum[:, cols]).astype(f32)
                    score = jnp.sum(q_rot[per_owner + j, :, cols].astype(f32) * k_new, axis=1, keepdims=True)
                    scores += [(2 * g + c, score[rows_of(g)] * score_scale) for g in range(groups)]
                new_tiles.append(packed(scores))
            for j in range(per_owner):
                h = own_head(w, j)
                for o in range(1, n_kv):
                    peer = kv_at(o)
                    at, stat_at = att_buf.at[peer, h], att_stat.at[peer, h]
                    remote(at, at, att_ss.at[0], att_rs.at[peer, h], "kv", peer).wait_recv()
                    remote(stat_at, stat_at, as_ss.at[0], as_rs.at[peer, h], "kv", peer).wait_recv()
                row_max = new_tiles[j]
                for s in range(n_kv):
                    row_max = jnp.maximum(row_max, att_stat[s, h])
                new_weight = jnp.exp(new_tiles[j] - row_max)
                total = new_weight
                scales = []
                for s in range(n_kv):
                    tile = att_stat[s, h]
                    scale = jnp.exp(tile - row_max)
                    total = total + scale * pltpu.roll(tile, LANES - MASS_LANE, 1)
                    scales.append(scale)
                share = 1.0 / total
                share = share * jnp.where(lane % 2 == 0, 1.0, -lam_ref[h])
                new_share = new_weight * share
                shares = [scale * share for scale in scales]
                log_buf[h] = row_max + jnp.log(total)
                pieces = []
                for g in range(groups):
                    at = 2 * g
                    piece = (new_share[:, at : at + 1] + new_share[:, at + 1 : at + 2]) * new_values[j][rows_of(g)]
                    for s in range(n_kv):
                        for c in range(2):
                            dst = slice(c * seqs + g * ROWS, c * seqs + (g + 1) * ROWS)
                            piece = piece + shares[s][:, at + c : at + c + 1] * att_buf[s, h, dst].astype(f32)
                    pieces.append(piece)
                difference = jnp.concatenate(pieces, axis=0)
                inv_head = lax.rsqrt(jnp.mean(difference * difference, axis=1, keepdims=True) + 1e-05)
                head_buf[h] = (difference * inv_head * hgain_ref[...]).astype(bf16)
                for copy in head_copies(h):
                    copy.start()

    for copy in wo_loads:
        copy.wait()
    head_order = [w * per_owner + j for j in range(per_owner) for w in range(2)]
    parts = [None] * n_tp
    for h in head_order:

        @pl.when(my_kv != first_owner + h // per_owner)
        def _(h=h):
            at = head_buf.at[h]
            remote(at, at, head_ss.at[h, 0], head_rs.at[h], "kv", kv_at(1)).wait_recv()

        attended = head_buf[h]
        for i in range(n_tp):
            term = jnp.dot(attended, wo_buf[i, h * vdim : (h + 1) * vdim], preferred_element_type=f32)
            parts[i] = term if parts[i] is None else parts[i] + term
    o_copies = []
    for i in range(n_tp - 1):
        o_send[i] = parts[i].astype(bf16)
        o_copies.append(send(o_send.at[i], o_recv.at[i], o_ss.at[i], o_rs.at[i], "tp", tp_at(i + 1)))
    sends += o_copies

    for h in range(heads):

        @pl.when(my_kv != first_owner + h // per_owner)
        def _(h=h):
            at = log_buf.at[h]
            remote(at, at, log_ss.at[h, 0], log_rs.at[h], "kv", kv_at(1)).wait_recv()

    pieces = []
    for g in range(groups):
        piece = jnp.zeros((ROWS, LANES), f32)
        for h in range(heads):
            tile = pltpu.roll(log_buf[h], (2 * h - 2 * g) % LANES, 1)
            piece = jnp.where((lane // 2) == h, tile, piece)
        pieces.append(piece)
    logs = jnp.concatenate(pieces, axis=0).T
    for h in range(heads):
        log_ref[h] = logs[2 * h : 2 * h + 2]

    result = parts[n_tp - 1].astype(bf16).astype(f32)
    for i, copy in enumerate(o_copies):
        copy.wait_recv()
        result = result + o_recv[i].astype(f32)
    out_ref[...] = result.astype(bf16)

    for copy in sends:
        copy.wait_send()
    for i in range(heads):
        if i < per_owner:
            for copy in att_copies(i):
                copy.wait_send()
        else:

            @pl.when(jnp.logical_not(is_owner))
            def _(i=i):
                for copy in att_copies(i):
                    copy.wait_send()

    for w in range(2):

        @pl.when(my_kv != first_owner + w)
        def _(w=w):
            new_stat_copy(w).wait_send()
            for j in range(per_owner):
                new_copies(w * per_owner + j).wait_send()

        @pl.when(my_kv == first_owner + w)
        def _(w=w):
            for j in range(per_owner):
                for copy in head_copies(own_head(w, j)):
                    copy.wait_send()


def hand_out(layer_in, logs_in, layer_out, logs_out):
    layer_out[...] = layer_in[...]
    logs_out[...] = logs_in[...]


def fused(
    n_kv,
    n_tp,
    tokens,
    norm_gain,
    query_weight,
    key_weight,
    value_weight,
    lambda_head,
    head_gain,
    out_weight,
    cache_keys,
    cache_values,
    lengths,
):
    seqs, tok_w = tokens.shape
    span = cache_keys.shape[1]
    depth, width = query_weight.shape
    heads = lambda_head.shape[0]
    out_w = out_weight.shape[1] // n_tp
    bf16, f32, i16 = jnp.bfloat16, jnp.float32, jnp.int16
    dma = pltpu.SemaphoreType.DMA
    anyspace = pl.BlockSpec(memory_space=pl.ANY)
    vmem = pl.BlockSpec(memory_space=pltpu.VMEM)
    k1, t1 = n_kv - 1, n_tp - 1
    operands = [
        pltpu.with_memory_space_constraint(a, pltpu.HBM)
        for a in (
            tokens,
            norm_gain.reshape(tok_w // LANES, LANES),
            query_weight,
            key_weight,
            value_weight,
            lambda_head,
            head_gain.reshape(1, VALUE_DIM),
            out_weight,
            cache_keys,
            cache_values,
            lengths,
        )
    ]
    layer, logs = pl.pallas_call(
        functools.partial(fused_kernel, n_kv, n_tp),
        out_shape=(pltpu.VMEM((seqs, out_w), bf16), pltpu.VMEM((heads, 2, seqs), f32)),
        in_specs=[anyspace] * len(operands),
        out_specs=(vmem, vmem),
        scratch_shapes=[
            pltpu.VMEM((n_tp, seqs, tok_w), bf16),
            pltpu.VMEM((n_tp, tok_w // LANES, LANES), bf16),
            pltpu.SMEM(lambda_head.shape, f32),
            pltpu.VMEM((1, VALUE_DIM), f32),
            pltpu.SMEM(lengths.shape, jnp.int32),
            pltpu.VMEM((depth, width), bf16),
            pltpu.VMEM((depth, width), bf16),
            pltpu.VMEM((depth, width), bf16),
            pltpu.VMEM((heads, seqs, span, VALUE_DIM), bf16),
            pltpu.VMEM((heads, seqs, span, VALUE_DIM), bf16),
            pltpu.VMEM((n_tp, out_weight.shape[0], out_w), bf16),
            pltpu.VMEM((n_kv, heads, seqs, VALUE_DIM), i16),
            pltpu.VMEM((n_kv, ROWS, LANES), bf16),
            pltpu.VMEM((heads, n_kv, seqs, VALUE_DIM), f32),
            pltpu.VMEM((heads, seqs, VALUE_DIM), bf16),
            pltpu.VMEM((n_kv, heads, seqs, 2 * VALUE_DIM), i16),
            pltpu.VMEM((n_kv, ROWS, LANES), bf16),
            pltpu.VMEM((n_kv, heads, 2 * seqs, VALUE_DIM), bf16),
            pltpu.VMEM((n_kv, heads, ROWS, LANES), f32),
            pltpu.VMEM((heads, seqs, VALUE_DIM), bf16),
            pltpu.VMEM((heads, ROWS, LANES), f32),
            pltpu.VMEM((t1, seqs, out_w), bf16),
            pltpu.VMEM((t1, seqs, out_w), bf16),
            dma((5,)),
            dma((3,)),
            dma((2 * heads,)),
            dma((n_tp,)),
            dma((2 * t1,)),
            dma((2 * t1,)),
            dma((heads, k1)),
            dma((n_kv, heads)),
            dma((k1,)),
            dma((n_kv,)),
            dma((heads,)),
            dma((n_kv, heads)),
            dma((2,)),
            dma((n_kv,)),
            dma((heads,)),
            dma((n_kv, heads)),
            dma((heads,)),
            dma((n_kv, heads)),
            dma((heads, k1)),
            dma((heads,)),
            dma((heads, k1)),
            dma((heads,)),
            dma((t1,)),
            dma((t1,)),
            pltpu.SemaphoreType.REGULAR,
            pltpu.SemaphoreType.REGULAR,
        ],
        compiler_params=pltpu.CompilerParams(
            collective_id=0, has_side_effects=True, vmem_limit_bytes=40 * 1024 * 1024
        ),
        name="decode_step",
    )(*operands)
    layer, logs = (pltpu.with_memory_space_constraint(a, pltpu.VMEM) for a in (layer, logs))
    layer, logs = pl.pallas_call(
        hand_out,
        out_shape=(
            jax.ShapeDtypeStruct((seqs, out_w), bf16),
            jax.ShapeDtypeStruct((heads, 2, seqs), f32),
        ),
        in_specs=(vmem, vmem),
        out_specs=(vmem, vmem),
        name="hand_out",
    )(layer, logs)
    return layer, logs.transpose(2, 0, 1)


def fits_fused(n_kv, n_tp, tokens, lambda_head, out_weight, cache_keys):
    seqs, tok_w = tokens.shape
    heads = lambda_head.shape[0]
    resident = 2 * (4 * out_weight.size + 2 * cache_keys.size)
    groups = seqs // ROWS
    return (
        heads == n_kv
        and n_kv > 2
        and n_kv % 2 == 0
        and n_tp > 1
        and seqs % ROWS == 0
        and tok_w % LANES == 0
        and (out_weight.shape[1] // n_tp) % LANES == 0
        and groups * max(2 * heads + SQUARE_LANES, 4 * heads) <= LANES
        and 2 * groups <= MASS_LANE
        and cache_keys.shape[1] % 16 == 0
        and resident <= 24 * 1024 * 1024
    )


def step(*args):
    n_kv, n_tp = lax.axis_size("kv"), lax.axis_size("tp")
    tokens, lambda_head, out_weight, cache_keys = args[0], args[5], args[7], args[8]
    if fits_fused(n_kv, n_tp, tokens, lambda_head, out_weight, cache_keys):
        return fused(n_kv, n_tp, *args)
    return on_device(*args)


def solution(mesh):
    in_specs = (
        P("grp", ("kv", "tp")),
        P(("kv", "tp")),
        P("kv", "tp"),
        P("kv", "tp"),
        P("kv", "tp"),
        P("tp"),
        P(),
        P("tp", "kv"),
        P("grp", "kv", "tp"),
        P("grp", "kv", "tp"),
        P("grp"),
    )
    out_specs = (P("grp", ("kv", "tp")), P("grp", "tp", None))
    return jax.shard_map(
        step, mesh=mesh, in_specs=in_specs, out_specs=out_specs, check_vma=False
    )
```

```python
import functools
import math

import jax
import jax.numpy as jnp
from jax import lax
from jax.experimental import pallas as pl
from jax.experimental.pallas import tpu as pltpu
from jax.sharding import PartitionSpec as P

D = 4096
HEAD_DIM = 128
VALUE_DIM = 256


def merged(part, axis, combine):
    gathered = jax.tree.map(lambda a: lax.all_gather(a, axis), part)

    def take(source):
        return jax.tree.map(lambda a: lax.dynamic_index_in_dim(a, source, 0, False), gathered)

    return lax.fori_loop(
        1, lax.axis_size(axis), lambda source, state: combine(state, take(source)), take(0)
    )


def rotate(vectors, lengths):
    half_dim = vectors.shape[-1] // 2
    freqs = jnp.power(
        jnp.float32(500000.0), -(jnp.arange(half_dim, dtype=jnp.float32) * 2.0 / vectors.shape[-1])
    )
    angles = lengths.astype(jnp.float32)[:, None] * freqs[None, :]
    cosine = jnp.cos(angles)[:, None, None, :]
    sine = jnp.sin(angles)[:, None, None, :]
    lower = vectors[..., :half_dim]
    upper = vectors[..., half_dim:]
    return jnp.concatenate([lower * cosine - upper * sine, upper * cosine + lower * sine], axis=-1)


def fold_maps(left_part, right_part):
    left_max, left_sum, left_out = left_part
    right_max, right_sum, right_out = right_part
    joint = jnp.maximum(left_max, right_max)
    left_scale = jnp.exp(left_max - joint)
    right_scale = jnp.exp(right_max - joint)
    return (
        joint,
        left_sum * left_scale + right_sum * right_scale,
        left_out * left_scale[..., None] + right_out * right_scale[..., None],
    )


def on_device(
    tokens,
    norm_gain,
    query_weight,
    key_weight,
    value_weight,
    lambda_head,
    head_gain,
    out_weight,
    cache_keys,
    cache_values,
    lengths,
):
    seq_count = tokens.shape[0]
    heads_loc = lambda_head.shape[0]
    token_block, gain_block = (
        lax.all_gather(tokens, "tp", axis=1, tiled=True),
        lax.all_gather(norm_gain, "tp", axis=0, tiled=True),
    )
    tok_float = token_block.astype(jnp.float32)
    scaled = (tok_float * gain_block.astype(jnp.float32)).astype(jnp.bfloat16)
    query_part = jnp.dot(scaled, query_weight, preferred_element_type=jnp.float32)
    key_part = jnp.dot(scaled, key_weight, preferred_element_type=jnp.float32)
    value_part = jnp.dot(scaled, value_weight, preferred_element_type=jnp.float32)
    local_squares = jnp.sum(tok_float * tok_float, axis=1)
    query_sum, key_sum, value_sum, row_squares = lax.psum(
        (query_part, key_part, value_part, local_squares), "kv"
    )
    inv_rms = lax.rsqrt(row_squares / D + 1e-06)[:, None]
    queries = rotate(
        (query_sum * inv_rms).reshape(seq_count, heads_loc, 2, HEAD_DIM), lengths
    ).astype(jnp.bfloat16)
    key_new = rotate(
        (key_sum * inv_rms).reshape(seq_count, heads_loc, 2, HEAD_DIM), lengths
    ).astype(jnp.bfloat16)
    value_new = (value_sum * inv_rms).astype(jnp.bfloat16).reshape(seq_count, heads_loc, VALUE_DIM)
    span_len = cache_keys.shape[1]
    positions = lax.axis_index("kv") * span_len + jnp.arange(span_len, dtype=jnp.int32)
    new_slot = positions[None, :] == lengths[:, None]
    before = positions[None, :] < lengths[:, None]
    visible = positions[None, :] <= lengths[:, None]
    score_scale = HEAD_DIM ** (-0.5)
    keys_four = cache_keys.reshape(seq_count, span_len, heads_loc, 2, HEAD_DIM)
    scores = (
        jnp.einsum("bhcd,bphcd->bhcp", queries, keys_four, preferred_element_type=jnp.float32)
        * score_scale
    )
    new_score = (
        jnp.einsum("bhcd,bhcd->bhc", queries, key_new, preferred_element_type=jnp.float32)
        * score_scale
    )
    scores = jnp.where(new_slot[:, None, None, :], new_score[..., None], scores)
    visible_four = visible[:, None, None, :]
    block_max = jnp.max(jnp.where(visible_four, scores, -1e30), axis=-1)
    weights = jnp.where(visible_four, jnp.exp(scores - block_max[..., None]), 0.0)
    block_sum = jnp.sum(weights, axis=-1)
    weights_low = weights.astype(jnp.bfloat16)
    cache_weights = jnp.where(before[:, None, None, :], weights_low, jnp.zeros((), jnp.bfloat16))
    values_four = cache_values.reshape(seq_count, span_len, heads_loc, VALUE_DIM)
    block_out = jnp.einsum(
        "bhcp,bphe->bhce", cache_weights, values_four, preferred_element_type=jnp.float32
    )
    weight_new = jnp.sum(
        jnp.where(new_slot[:, None, None, :], weights_low.astype(jnp.float32), 0.0), axis=-1
    )
    block_out = block_out + weight_new[..., None] * value_new.astype(jnp.float32)[:, :, None, :]
    row_max, weight_total, combined = merged((block_max, block_sum, block_out), "kv", fold_maps)
    map_out = combined / weight_total[..., None]
    difference = map_out[:, :, 0] - lambda_head[None, :, None] * map_out[:, :, 1]
    inv_head = lax.rsqrt(jnp.mean(difference * difference, axis=-1, keepdims=True) + 1e-05)
    attended = (
        (difference * inv_head * head_gain)
        .astype(jnp.bfloat16)
        .reshape(seq_count, heads_loc * VALUE_DIM)
    )
    log_sums = row_max + jnp.log(weight_total)
    partial_value = jnp.dot(attended, out_weight, preferred_element_type=jnp.float32)
    layer_out = lax.psum_scatter(
        partial_value.astype(jnp.bfloat16), "tp", scatter_dimension=1, tiled=True
    )
    return (layer_out, log_sums)


MESH = pl.DeviceIdType.MESH
LANES = 128
ROWS = 8


STEPS = 32767.0
ROUND_UP = 1.0 + 2.0**-7
SQUARE_LANES = 3
MASS_LANE = 64


def fused_kernel(
    n_kv,
    n_tp,
    tok_hbm,
    gain_hbm,
    wq_hbm,
    wk_hbm,
    wv_hbm,
    lam_hbm,
    hgain_hbm,
    wo_hbm,
    ck_hbm,
    cv_hbm,
    len_hbm,
    out_ref,
    log_ref,
    tok_buf,
    gain_buf,
    lam_ref,
    hgain_ref,
    len_ref,
    wq_buf,
    wk_buf,
    wv_buf,
    k_buf,
    v_buf,
    wo_buf,
    q_buf,
    q_stat,
    q_scale,
    q_rot,
    new_buf,
    new_stat,
    att_buf,
    att_stat,
    head_buf,
    log_buf,
    o_send,
    o_recv,
    own_sem,
    w_sem,
    kv_sem,
    wo_sem,
    tok_ss,
    tok_rs,
    q_ss,
    q_rs,
    qs_ss,
    qs_rs,
    new_ss,
    new_rs,
    ns_ss,
    ns_rs,
    att_ss,
    att_rs,
    as_ss,
    as_rs,
    head_ss,
    head_rs,
    log_ss,
    log_rs,
    o_ss,
    o_rs,
    plane_sem,
    all_sem,
):
    f32, bf16, i32, i16 = jnp.float32, jnp.bfloat16, jnp.int32, jnp.int16
    my_kv, my_tp = lax.axis_index("kv"), lax.axis_index("tp")
    seqs, tok_w = tok_hbm.shape
    span = ck_hbm.shape[1]
    vdim = VALUE_DIM
    heads = n_kv
    per_owner = heads // 2
    groups = seqs // ROWS
    out_w = out_ref.shape[1]
    first_owner = n_kv // 2 - 1
    low_side = my_kv <= first_owner
    is_owner = (my_kv == first_owner) | (my_kv == first_owner + 1)
    far_owner = jnp.where(low_side, 1, 0)
    stride = 2 * heads + SQUARE_LANES
    new_stride = 4 * heads

    def tp_at(offset):
        return lax.rem(my_tp + offset, n_tp)

    def kv_at(offset):
        return lax.rem(my_kv + offset, n_kv)

    def kv_peer(t):
        down = n_kv - 1 - t
        down = jnp.where(down <= my_kv, down - 1, down)
        up = jnp.where(t >= my_kv, t + 1, t)
        return jnp.where(low_side, down, up)

    def slot_head(i, far):
        owner = far if i < per_owner else 1 - far
        return owner * per_owner + i % per_owner

    def remote(src, dst, ss, rs, axis, peer):
        return pltpu.make_async_remote_copy(
            src_ref=src, dst_ref=dst, send_sem=ss, recv_sem=rs, device_id={axis: peer}, device_id_type=MESH
        )

    def send(*args):
        copy = remote(*args)
        copy.start()
        return copy

    def load(src, dst, sem):
        copy = pltpu.make_async_copy(src, dst, sem)
        copy.start()
        return copy

    barrier = pltpu.get_barrier_semaphore()
    gate, leader = n_tp - 1, n_tp - 2
    is_gate = my_tp == gate

    def signal(sem, axis, peer):
        pl.semaphore_signal(sem, inc=1, device_id={axis: peer}, device_id_type=MESH)

    for t in range(n_tp):
        if t != gate:

            @pl.when(my_tp != t)
            def _(t=t):
                signal(barrier, "tp", t)

    tok_load = load(tok_hbm, tok_buf.at[my_tp], own_sem.at[0])
    gain_load = load(gain_hbm, gain_buf.at[my_tp], own_sem.at[1])
    len_load = load(len_hbm, len_ref, own_sem.at[2])
    lam_load = load(lam_hbm, lam_ref, own_sem.at[3])
    hgain_load = load(hgain_hbm, hgain_ref, own_sem.at[4])
    tok_load.wait()
    gain_load.wait()
    w_loads = [
        load(w, buf, w_sem.at[m])
        for m, (w, buf) in enumerate(((wq_hbm, wq_buf), (wk_hbm, wk_buf), (wv_hbm, wv_buf)))
    ]
    kv_loads = []
    for i in range(heads):
        cols = pl.ds(pl.multiple_of(slot_head(i, far_owner) * vdim, vdim), vdim)
        kv_loads.append(
            (
                load(ck_hbm.at[:, :, cols], k_buf.at[i], kv_sem.at[2 * i]),
                load(cv_hbm.at[:, :, cols], v_buf.at[i], kv_sem.at[2 * i + 1]),
            )
        )
    wo_loads = []
    for i in range(n_tp):
        cols = pl.ds(pl.multiple_of(tp_at(i + 1) * out_w, out_w), out_w)
        wo_loads.append(load(wo_hbm.at[:, cols], wo_buf.at[i], wo_sem.at[i]))


    @pl.when(jnp.logical_not(is_gate))
    def _():
        pl.semaphore_wait(barrier, n_tp - 1)

    @pl.when(my_tp == leader)
    def _():
        signal(plane_sem, "tp", gate)

    @pl.when(is_gate)
    def _():
        pl.semaphore_wait(plane_sem, 1)
        for offset in range(1, n_kv):
            signal(barrier, "kv", kv_at(offset))

    sends = []
    tok_copies = []
    for o in range(n_tp - 1, 0, -1):
        peer = tp_at(o)
        for m, buf in enumerate((tok_buf, gain_buf)):
            tok_copies.append(
                send(
                    buf.at[my_tp],
                    buf.at[my_tp],
                    tok_ss.at[2 * o - 2 + m],
                    tok_rs.at[2 * o - 2 + m],
                    "tp",
                    peer,
                )
            )
    sends += tok_copies

    @pl.when(is_gate)
    def _():
        pl.semaphore_wait(barrier, n_kv - 1)
        for t in range(n_tp):
            if t != gate:
                signal(all_sem, "tp", t)

    len_load.wait()
    lane_id = lax.broadcasted_iota(i32, (seqs, LANES), 1)
    row_id = lax.broadcasted_iota(i32, (seqs, LANES), 0)
    lens = jnp.zeros((seqs, LANES), i32)
    for b in range(seqs):
        lens = jnp.where(row_id == b, len_ref[b], lens)
    half = HEAD_DIM // 2
    upper = lane_id >= half
    freq_id = jnp.where(upper, lane_id - half, lane_id).astype(f32)
    angles = lens.astype(f32) * jnp.exp(freq_id * (-2.0 * math.log(500000.0) / HEAD_DIM))
    cosine = jnp.cos(angles)
    sine = jnp.sin(angles)
    sine = jnp.where(upper, sine, -sine)

    def rotated(x):
        return (x * cosine + pltpu.roll(x, half, 1) * sine).astype(bf16)

    lane = lax.broadcasted_iota(i32, (ROWS, LANES), 1)

    def packed(columns):
        tile = jnp.zeros((ROWS, LANES), f32)
        for at, column in columns:
            tile = jnp.where(lane == at, column, tile)
        return tile

    def coded(x):
        top = jnp.maximum(jnp.max(jnp.abs(x), axis=1, keepdims=True), 1e-30)
        scale = (top * (ROUND_UP / STEPS)).astype(bf16).astype(f32)
        return jnp.round(x * (1.0 / scale)).astype(i32).astype(i16), scale

    def thirds(x):
        high = x.astype(bf16).astype(f32)
        middle = (x - high).astype(bf16).astype(f32)
        return high, middle, x - high - middle

    def rows_of(g):
        return slice(g * ROWS, (g + 1) * ROWS)

    def decoded(codes, tile, width, at):
        value = codes.astype(i32).astype(f32)
        pieces = []
        for g in range(groups):
            rows = []
            for c in range(width):
                scale = tile[:, g * new_stride + at + c : g * new_stride + at + c + 1]
                rows.append(value[rows_of(g), c * LANES : (c + 1) * LANES] * scale)
            pieces.append(jnp.concatenate(rows, axis=1))
        return jnp.concatenate(pieces, axis=0)

    for copy in tok_copies:
        copy.wait_recv()
    squares = jnp.zeros((seqs, 1), f32)
    scaled_parts = []
    for s in range(n_tp):
        tok = tok_buf[s].astype(f32)
        squares = squares + jnp.sum(tok * tok, axis=1, keepdims=True)
        gain = gain_buf[s].astype(f32)
        gain = jnp.concatenate([gain[r : r + 1] for r in range(tok_w // LANES)], axis=1)
        scaled_parts.append((tok * gain).astype(bf16))
    scaled = jnp.concatenate(scaled_parts, axis=1)

    w_loads[0].wait()
    square_parts = thirds(squares)
    columns = [
        (g * stride + 2 * heads + m, third[rows_of(g)]) for m, third in enumerate(square_parts) for g in range(groups)
    ]
    for h in range(heads):
        part = jnp.dot(scaled, wq_buf[:, h * vdim : (h + 1) * vdim], preferred_element_type=f32)
        for c in range(2):
            cols = slice(c * HEAD_DIM, (c + 1) * HEAD_DIM)
            code, scale = coded(part[:, cols])
            q_buf[my_kv, h, :, cols] = code
            columns += [(g * stride + 2 * h + c, scale[rows_of(g)]) for g in range(groups)]
    q_stat[my_kv] = packed(columns).astype(bf16)

    @pl.when(jnp.logical_not(is_gate))
    def _():
        pl.semaphore_wait(all_sem, 1)

    for t in range(n_kv - 1):
        at = q_stat.at[my_kv]
        sends.append(send(at, at, qs_ss.at[t], qs_rs.at[my_kv], "kv", kv_peer(t)))
    for i in range(heads):
        for t in range(n_kv - 1):
            peer = kv_peer(t)
            h = slot_head(i, jnp.where(peer <= first_owner, 1, 0))
            at = q_buf.at[my_kv, h]
            sends.append(send(at, at, q_ss.at[i, t], q_rs.at[my_kv, h], "kv", peer))

    columns = []
    w_loads[1].wait()
    w_loads[2].wait()
    for m, w in enumerate((wk_buf, wv_buf)):
        part = jnp.dot(scaled, w[...], preferred_element_type=f32)
        for j in range(2 * heads):
            code, scale = coded(part[:, j * HEAD_DIM : (j + 1) * HEAD_DIM])
            lo = m * vdim + (j % 2) * HEAD_DIM
            new_buf[my_kv, j // 2, :, lo : lo + HEAD_DIM] = code
            columns.append((m, j, scale))
    new_stat[my_kv] = packed(
        [(g * new_stride + 2 * heads * m + j, scale[rows_of(g)]) for m, j, scale in columns for g in range(groups)]
    ).astype(bf16)

    def new_copies(h):
        at = new_buf.at[my_kv, h]
        return remote(at, at, new_ss.at[h], new_rs.at[my_kv, h], "kv", first_owner + h // per_owner)

    def new_stat_copy(w):
        at = new_stat.at[my_kv]
        return remote(at, at, ns_ss.at[w], ns_rs.at[my_kv], "kv", first_owner + w)

    score_scale = HEAD_DIM ** (-0.5)
    wide = ROWS * span
    col = lax.broadcasted_iota(i32, (2 * ROWS, wide), 1)
    row = lax.broadcasted_iota(i32, (2 * ROWS, wide), 0)
    start = (row % ROWS) * span
    masks = []
    for g in range(groups):
        len_g = lens[rows_of(g), 0:1]
        len_g = jnp.concatenate([len_g, len_g], axis=0)
        limit = jnp.minimum(len_g - my_kv * span, span)
        masks.append((col >= start) & (col - start < limit))
    lane_q = lax.broadcasted_iota(i32, (ROWS, vdim), 1)
    contract_last = (((1,), (1,)), ((), ()))

    def att_copies(i):
        h = slot_head(i, far_owner)
        owner = first_owner + (far_owner if i < per_owner else 1 - far_owner)
        at, stat_at = att_buf.at[my_kv, h], att_stat.at[my_kv, h]
        return [
            remote(at, at, att_ss.at[i], att_rs.at[my_kv, h], "kv", owner),
            remote(stat_at, stat_at, as_ss.at[i], as_rs.at[my_kv, h], "kv", owner),
        ]

    for o in range(1, n_kv):
        peer = kv_at(o)
        at = q_stat.at[peer]
        remote(at, at, qs_ss.at[o - 1], qs_rs.at[peer], "kv", peer).wait_recv()
    inv_rms = []
    for g in range(groups):
        total = jnp.zeros((ROWS, 1), f32)
        for s in range(n_kv):
            tile = q_stat[s].astype(f32)
            for m in range(SQUARE_LANES):
                at = g * stride + 2 * heads + m
                total = total + tile[:, at : at + 1]
        inv_rms.append(lax.rsqrt(total / (tok_w * n_tp * n_kv) + 1e-06))
    inv_rms = jnp.concatenate(inv_rms, axis=0)

    def spread_scales(slots):
        for i in slots:
            h = slot_head(i, far_owner)
            for s in range(n_kv):
                tile = pltpu.roll(q_stat[s].astype(f32), lax.rem(LANES - 2 * h, LANES), 1)
                for c in range(2):
                    scale = jnp.concatenate([tile[:, g * stride + c : g * stride + c + 1] for g in range(groups)], axis=0)
                    cols = slice(c * HEAD_DIM, (c + 1) * HEAD_DIM)
                    q_scale[i, s, :, cols] = jnp.broadcast_to(scale * inv_rms, (seqs, HEAD_DIM))

    def arrived(i):
        h = slot_head(i, far_owner)
        for o in range(1, n_kv):
            peer = kv_at(o)
            at = q_buf.at[peer, h]
            remote(at, at, q_ss.at[i, o - 1], q_rs.at[peer, h], "kv", peer).wait_recv()
        kv_loads[i][0].wait()
        kv_loads[i][1].wait()

    def attend(slots):
        jobs = [(i, g) for i in slots for g in range(groups)]
        queries, scores, tops, weights, masses, outs = {}, {}, {}, {}, {}, {}
        for i in slots:
            h = slot_head(i, far_owner)
            total = jnp.zeros((seqs, vdim), f32)
            for s in range(n_kv):
                total = total + q_buf[s, h].astype(i32).astype(f32) * q_scale[i, s]
            maps = [rotated(total[:, c * HEAD_DIM : (c + 1) * HEAD_DIM]) for c in range(2)]
            for c in range(2):
                q_rot[i, :, c * HEAD_DIM : (c + 1) * HEAD_DIM] = maps[c]
            queries[i] = jnp.concatenate([m.astype(f32) for m in maps], axis=1)
        for i, g in jobs:
            q_g = queries[i][rows_of(g)]
            lhs = jnp.concatenate(
                [jnp.where(lane_q < HEAD_DIM, q_g, 0.0), jnp.where(lane_q < HEAD_DIM, 0.0, q_g)], axis=0
            ).astype(bf16)
            keys = k_buf[i, rows_of(g)].reshape(wide, vdim)
            scores[i, g] = lax.dot_general(lhs, keys, contract_last, preferred_element_type=f32)
        for i, g in jobs:
            scores[i, g] = jnp.where(masks[g], scores[i, g] * score_scale, -1e30)
            tops[i, g] = jnp.max(scores[i, g], axis=1, keepdims=True)
        for i, g in jobs:
            weights[i, g] = jnp.where(masks[g], jnp.exp(scores[i, g] - tops[i, g]), 0.0)
            masses[i, g] = jnp.sum(weights[i, g], axis=1, keepdims=True)
        for i, g in jobs:
            values = v_buf[i, rows_of(g)].reshape(wide, vdim)
            outs[i, g] = jnp.dot(weights[i, g].astype(bf16), values, preferred_element_type=f32)
        for i in slots:
            h = slot_head(i, far_owner)
            stats = []
            for g in range(groups):
                out = outs[i, g].astype(bf16)
                for c in range(2):
                    part = slice(c * ROWS, (c + 1) * ROWS)
                    att_buf[my_kv, h, c * seqs + g * ROWS : c * seqs + (g + 1) * ROWS] = out[part]
                    stats.append((2 * g + c, tops[i, g][part]))
                    stats.append((MASS_LANE + 2 * g + c, masses[i, g][part]))
            att_stat[my_kv, h] = packed(stats)

    def deliver(i):
        if i < per_owner:
            for copy in att_copies(i):
                copy.start()
        else:

            @pl.when(jnp.logical_not(is_owner))
            def _():
                for copy in att_copies(i):
                    copy.start()

    turns = [(i,) for i in range(heads)]
    spread_scales(range(per_owner))
    for j, turn in enumerate(turns):
        for i in turn:
            arrived(i)
        if j == 0:
            for w in range(2):

                @pl.when(my_kv != first_owner + w)
                def _(w=w):
                    new_stat_copy(w).start()
                    for k in range(per_owner):
                        new_copies(w * per_owner + k).start()

        if j == 0:
            spread_scales(range(per_owner, heads))
        attend(turn)
        for i in turn:
            deliver(i)

    lam_load.wait()
    hgain_load.wait()

    def head_copies(h):
        at, log_at = head_buf.at[h], log_buf.at[h]
        made = []
        for o in range(1, n_kv):
            peer = kv_at(o)
            made.append(remote(at, at, head_ss.at[h, o - 1], head_rs.at[h], "kv", peer))
        for o in range(1, n_kv):
            peer = kv_at(o)
            made.append(remote(log_at, log_at, log_ss.at[h, o - 1], log_rs.at[h], "kv", peer))
        return made

    def own_head(w, j):
        return w * per_owner + j

    for w in range(2):

        @pl.when(my_kv == first_owner + w)
        def _(w=w):
            for o in range(1, n_kv):
                peer = kv_at(o)
                at = new_stat.at[peer]
                remote(at, at, ns_ss.at[w], ns_rs.at[peer], "kv", peer).wait_recv()
            new_tiles, new_values = [], []
            for j in range(per_owner):
                h = own_head(w, j)
                for o in range(1, n_kv):
                    peer = kv_at(o)
                    at = new_buf.at[peer, h]
                    remote(at, at, new_ss.at[h], new_rs.at[peer, h], "kv", peer).wait_recv()
                k_sum = jnp.zeros((seqs, vdim), f32)
                v_sum = jnp.zeros((seqs, vdim), f32)
                for s in range(n_kv):
                    codes = new_buf[s, h]
                    tile = new_stat[s].astype(f32)
                    k_sum = k_sum + decoded(codes[:, :vdim], tile, 2, 2 * h)
                    v_sum = v_sum + decoded(codes[:, vdim:], tile, 2, 2 * (heads + h))
                k_sum = k_sum * inv_rms
                new_values.append((v_sum * inv_rms).astype(bf16).astype(f32))
                scores = []
                for c in range(2):
                    cols = slice(c * HEAD_DIM, (c + 1) * HEAD_DIM)
                    k_new = rotated(k_sum[:, cols]).astype(f32)
                    score = jnp.sum(q_rot[per_owner + j, :, cols].astype(f32) * k_new, axis=1, keepdims=True)
                    scores += [(2 * g + c, score[rows_of(g)] * score_scale) for g in range(groups)]
                new_tiles.append(packed(scores))
            for j in range(per_owner):
                h = own_head(w, j)
                for o in range(1, n_kv):
                    peer = kv_at(o)
                    at, stat_at = att_buf.at[peer, h], att_stat.at[peer, h]
                    remote(at, at, att_ss.at[0], att_rs.at[peer, h], "kv", peer).wait_recv()
                    remote(stat_at, stat_at, as_ss.at[0], as_rs.at[peer, h], "kv", peer).wait_recv()
                row_max = new_tiles[j]
                for s in range(n_kv):
                    row_max = jnp.maximum(row_max, att_stat[s, h])
                new_weight = jnp.exp(new_tiles[j] - row_max)
                total = new_weight
                scales = []
                for s in range(n_kv):
                    tile = att_stat[s, h]
                    scale = jnp.exp(tile - row_max)
                    total = total + scale * pltpu.roll(tile, LANES - MASS_LANE, 1)
                    scales.append(scale)
                share = 1.0 / total
                share = share * jnp.where(lane % 2 == 0, 1.0, -lam_ref[h])
                new_share = new_weight * share
                shares = [scale * share for scale in scales]
                log_buf[h] = row_max + jnp.log(total)
                pieces = []
                for g in range(groups):
                    at = 2 * g
                    piece = (new_share[:, at : at + 1] + new_share[:, at + 1 : at + 2]) * new_values[j][rows_of(g)]
                    for s in range(n_kv):
                        for c in range(2):
                            dst = slice(c * seqs + g * ROWS, c * seqs + (g + 1) * ROWS)
                            piece = piece + shares[s][:, at + c : at + c + 1] * att_buf[s, h, dst].astype(f32)
                    pieces.append(piece)
                difference = jnp.concatenate(pieces, axis=0)
                inv_head = lax.rsqrt(jnp.mean(difference * difference, axis=1, keepdims=True) + 1e-05)
                head_buf[h] = (difference * inv_head * hgain_ref[...]).astype(bf16)
                for copy in head_copies(h):
                    copy.start()

    for copy in wo_loads:
        copy.wait()
    head_order = [w * per_owner + j for j in range(per_owner) for w in range(2)]
    parts = [None] * n_tp
    for h in head_order:

        @pl.when(my_kv != first_owner + h // per_owner)
        def _(h=h):
            at = head_buf.at[h]
            remote(at, at, head_ss.at[h, 0], head_rs.at[h], "kv", kv_at(1)).wait_recv()

        attended = head_buf[h]
        for i in range(n_tp):
            term = jnp.dot(attended, wo_buf[i, h * vdim : (h + 1) * vdim], preferred_element_type=f32)
            parts[i] = term if parts[i] is None else parts[i] + term
    o_copies = []
    for i in range(n_tp - 1):
        o_send[i] = parts[i].astype(bf16)
        o_copies.append(send(o_send.at[i], o_recv.at[i], o_ss.at[i], o_rs.at[i], "tp", tp_at(i + 1)))
    sends += o_copies

    for h in range(heads):

        @pl.when(my_kv != first_owner + h // per_owner)
        def _(h=h):
            at = log_buf.at[h]
            remote(at, at, log_ss.at[h, 0], log_rs.at[h], "kv", kv_at(1)).wait_recv()

    pieces = []
    for g in range(groups):
        piece = jnp.zeros((ROWS, LANES), f32)
        for h in range(heads):
            tile = pltpu.roll(log_buf[h], (2 * h - 2 * g) % LANES, 1)
            piece = jnp.where((lane // 2) == h, tile, piece)
        pieces.append(piece)
    logs = jnp.concatenate(pieces, axis=0).T
    for h in range(heads):
        log_ref[h] = logs[2 * h : 2 * h + 2]

    result = parts[n_tp - 1].astype(bf16).astype(f32)
    for i, copy in enumerate(o_copies):
        copy.wait_recv()
        result = result + o_recv[i].astype(f32)
    out_ref[...] = result.astype(bf16)

    for copy in sends:
        copy.wait_send()
    for i in range(heads):
        if i < per_owner:
            for copy in att_copies(i):
                copy.wait_send()
        else:

            @pl.when(jnp.logical_not(is_owner))
            def _(i=i):
                for copy in att_copies(i):
                    copy.wait_send()

    for w in range(2):

        @pl.when(my_kv != first_owner + w)
        def _(w=w):
            new_stat_copy(w).wait_send()
            for j in range(per_owner):
                new_copies(w * per_owner + j).wait_send()

        @pl.when(my_kv == first_owner + w)
        def _(w=w):
            for j in range(per_owner):
                for copy in head_copies(own_head(w, j)):
                    copy.wait_send()


def hand_out(layer_in, logs_in, layer_out, logs_out):
    layer_out[...] = layer_in[...]
    logs_out[...] = logs_in[...]


def fused(
    n_kv,
    n_tp,
    tokens,
    norm_gain,
    query_weight,
    key_weight,
    value_weight,
    lambda_head,
    head_gain,
    out_weight,
    cache_keys,
    cache_values,
    lengths,
):
    seqs, tok_w = tokens.shape
    span = cache_keys.shape[1]
    depth, width = query_weight.shape
    heads = lambda_head.shape[0]
    out_w = out_weight.shape[1] // n_tp
    bf16, f32, i16 = jnp.bfloat16, jnp.float32, jnp.int16
    dma = pltpu.SemaphoreType.DMA
    anyspace = pl.BlockSpec(memory_space=pl.ANY)
    vmem = pl.BlockSpec(memory_space=pltpu.VMEM)
    k1, t1 = n_kv - 1, n_tp - 1
    operands = [
        pltpu.with_memory_space_constraint(a, pltpu.HBM)
        for a in (
            tokens,
            norm_gain.reshape(tok_w // LANES, LANES),
            query_weight,
            key_weight,
            value_weight,
            lambda_head,
            head_gain.reshape(1, VALUE_DIM),
            out_weight,
            cache_keys,
            cache_values,
            lengths,
        )
    ]
    layer, logs = pl.pallas_call(
        functools.partial(fused_kernel, n_kv, n_tp),
        out_shape=(pltpu.VMEM((seqs, out_w), bf16), pltpu.VMEM((heads, 2, seqs), f32)),
        in_specs=[anyspace] * len(operands),
        out_specs=(vmem, vmem),
        scratch_shapes=[
            pltpu.VMEM((n_tp, seqs, tok_w), bf16),
            pltpu.VMEM((n_tp, tok_w // LANES, LANES), bf16),
            pltpu.SMEM(lambda_head.shape, f32),
            pltpu.VMEM((1, VALUE_DIM), f32),
            pltpu.SMEM(lengths.shape, jnp.int32),
            pltpu.VMEM((depth, width), bf16),
            pltpu.VMEM((depth, width), bf16),
            pltpu.VMEM((depth, width), bf16),
            pltpu.VMEM((heads, seqs, span, VALUE_DIM), bf16),
            pltpu.VMEM((heads, seqs, span, VALUE_DIM), bf16),
            pltpu.VMEM((n_tp, out_weight.shape[0], out_w), bf16),
            pltpu.VMEM((n_kv, heads, seqs, VALUE_DIM), i16),
            pltpu.VMEM((n_kv, ROWS, LANES), bf16),
            pltpu.VMEM((heads, n_kv, seqs, VALUE_DIM), f32),
            pltpu.VMEM((heads, seqs, VALUE_DIM), bf16),
            pltpu.VMEM((n_kv, heads, seqs, 2 * VALUE_DIM), i16),
            pltpu.VMEM((n_kv, ROWS, LANES), bf16),
            pltpu.VMEM((n_kv, heads, 2 * seqs, VALUE_DIM), bf16),
            pltpu.VMEM((n_kv, heads, ROWS, LANES), f32),
            pltpu.VMEM((heads, seqs, VALUE_DIM), bf16),
            pltpu.VMEM((heads, ROWS, LANES), f32),
            pltpu.VMEM((t1, seqs, out_w), bf16),
            pltpu.VMEM((t1, seqs, out_w), bf16),
            dma((5,)),
            dma((3,)),
            dma((2 * heads,)),
            dma((n_tp,)),
            dma((2 * t1,)),
            dma((2 * t1,)),
            dma((heads, k1)),
            dma((n_kv, heads)),
            dma((k1,)),
            dma((n_kv,)),
            dma((heads,)),
            dma((n_kv, heads)),
            dma((2,)),
            dma((n_kv,)),
            dma((heads,)),
            dma((n_kv, heads)),
            dma((heads,)),
            dma((n_kv, heads)),
            dma((heads, k1)),
            dma((heads,)),
            dma((heads, k1)),
            dma((heads,)),
            dma((t1,)),
            dma((t1,)),
            pltpu.SemaphoreType.REGULAR,
            pltpu.SemaphoreType.REGULAR,
        ],
        compiler_params=pltpu.CompilerParams(
            collective_id=0,
            has_side_effects=True,
            vmem_limit_bytes=40 * 1024 * 1024,
        ),
        name="decode_step",
    )(*operands)
    layer, logs = (pltpu.with_memory_space_constraint(a, pltpu.VMEM) for a in (layer, logs))
    layer, logs = pl.pallas_call(
        hand_out,
        out_shape=(
            jax.ShapeDtypeStruct((seqs, out_w), bf16),
            jax.ShapeDtypeStruct((heads, 2, seqs), f32),
        ),
        in_specs=(vmem, vmem),
        out_specs=(vmem, vmem),
        name="hand_out",
    )(layer, logs)
    return layer, logs.transpose(2, 0, 1)


def fits_fused(n_kv, n_tp, tokens, lambda_head, out_weight, cache_keys):
    seqs, tok_w = tokens.shape
    heads = lambda_head.shape[0]
    resident = 2 * (4 * out_weight.size + 2 * cache_keys.size)
    groups = seqs // ROWS
    return (
        heads == n_kv
        and n_kv > 2
        and n_kv % 2 == 0
        and n_tp > 1
        and seqs % ROWS == 0
        and tok_w % LANES == 0
        and (out_weight.shape[1] // n_tp) % LANES == 0
        and groups * max(2 * heads + SQUARE_LANES, 4 * heads) <= LANES
        and 2 * groups <= MASS_LANE
        and cache_keys.shape[1] % 16 == 0
        and resident <= 24 * 1024 * 1024
    )


def step(*args):
    n_kv, n_tp = lax.axis_size("kv"), lax.axis_size("tp")
    tokens, lambda_head, out_weight, cache_keys = args[0], args[5], args[7], args[8]
    if fits_fused(n_kv, n_tp, tokens, lambda_head, out_weight, cache_keys):
        return fused(n_kv, n_tp, *args)
    return on_device(*args)


def solution(mesh):
    in_specs = (
        P("grp", ("kv", "tp")),
        P(("kv", "tp")),
        P("kv", "tp"),
        P("kv", "tp"),
        P("kv", "tp"),
        P("tp"),
        P(),
        P("tp", "kv"),
        P("grp", "kv", "tp"),
        P("grp", "kv", "tp"),
        P("grp"),
    )
    out_specs = (P("grp", ("kv", "tp")), P("grp", "tp", None))
    return jax.shard_map(
        step, mesh=mesh, in_specs=in_specs, out_specs=out_specs, check_vma=False
    )
```
